512 devices in a mesh: ep: 32 (over z, x), tp: 16 (over y, core).
Axes of the slice: x: 4, y: 8, z: 8, core: 2. Of those that a mesh axis runs over, the one named last changes fastest.
Arguments:
- mix_input: bfloat16 [16384, 2048], P('ep', 'tp'), may hold values from -6 to 6
- mix_weight: bfloat16 [2048, 4096], P(None, 'tp'), may hold values from -0.125 to 0.125
- expert_input: bfloat16 [4096, 4096], P('ep', 'tp'), may hold values from -4500 to 4500
- expert_index: int32 [4096, 2], P('ep'), may hold values from 0 to 31, as said below
- route_share: float32 [4096, 2], P('ep'), may hold values from 0.1 to 1
- norm_gain: float32 [4096], replicated, may hold values from 0.1 to 1.9
- gate_weight: bfloat16 [32, 4096, 2048], P('ep', None, 'tp'), may hold values from -0.09375 to 0.09375
- up_weight: bfloat16 [32, 4096, 2048], P('ep', None, 'tp'), may hold values from -0.09375 to 0.09375
- down_weight: bfloat16 [32, 2048, 4096], P('ep', None, 'tp'), may hold values from -0.125 to 0.125
Outputs:
- mixed_rows: bfloat16 [16384, 4096], P('ep', 'tp')
- expert_rows: bfloat16 [4096, 4096], P('ep', 'tp')
The draws below stay inside these ranges and needn't reach their ends.
Inputs may be any that keep to these rules, and one draw needn't show every extreme that they name: `expert_index`: each row names 2 different experts. Within each aligned block of 128 rows (the rows of one index of ep) no expert is named by more than 16 rows, and one expert, the same in every block, is named by exactly 16 rows.
All inputs are finite; a program needn't handle non-finite values.
Results may differ from the reference program's by a relative error of at most 0.007.
Values may be sent and summed in bfloat16 or wider, within the bound.
A program may use at most 64 MiB of HBM per device.

```python
import math
from functools import partial
import jax
import jax.numpy as jnp
from jax import lax

D = 4096
POOL = 2048
FF = 2048
TOP = 2
TOK_EXP = 128
EXPERTS = 32
CAP = 16
TOKENS_MIX = 16384
TOKENS_EXP = 4096
N_EP = 32


def draw_expert_input(key, part):
    key_cols, key_rows, key_noise = jax.random.split(key, 3)
    column = jnp.arange(D, dtype=jnp.float32) / (D - 1)
    col_scale = jnp.exp(math.log(3.0) * column + jax.random.uniform(key_cols, (D,), jnp.float32, 0.0, math.log(10.0)))
    noise = jnp.clip(jax.random.normal(key_noise, (TOKENS_EXP, D), jnp.float32), -5.0, 5.0)
    row_scale = jnp.exp(jax.random.uniform(key_rows, (TOKENS_EXP, 1), jnp.float32, 0.0, math.log(10.0)))
    return (noise * col_scale[None, :] * row_scale).astype(jnp.bfloat16)


def draw_expert_index(key, part):
    key_full, key_rest = jax.random.split(key)
    favored = jax.random.randint(key_full, (), 0, EXPERTS)

    def one_block(block_key):
        key_order, key_rows, key_flip = jax.random.split(block_key, 3)
        others = jax.random.permutation(key_order, EXPERTS - 1).astype(jnp.int32)
        others = others + (others >= favored).astype(jnp.int32)
        row_number = jnp.arange(TOK_EXP, dtype=jnp.int32)
        first = jnp.where(row_number < CAP, favored, others[2 * row_number % (EXPERTS - 1)])
        second = jnp.where(row_number < CAP, others[row_number % (EXPERTS - 1)], others[(2 * row_number + 1) % (EXPERTS - 1)])
        flipped = jax.random.randint(key_flip, (TOK_EXP,), 0, 2)
        pairs = jnp.stack([jnp.where(flipped == 1, second, first), jnp.where(flipped == 1, first, second)], axis=1)
        shuffle = jax.random.permutation(key_rows, TOK_EXP)
        return pairs[shuffle]
    blocks = jax.vmap(one_block)(jax.random.split(key_rest, N_EP))
    return blocks.reshape(N_EP * TOK_EXP, 2).astype(jnp.int32)


def levels(own_key, shape, cuts, least, high):
    gain = 1.0
    for dim, shards_of in cuts:
        draws = jax.random.uniform(jax.random.fold_in(jax.random.fold_in(own_key, 6), dim), (shards_of,), jnp.float32, least / len(cuts), high / len(cuts))
        gain = gain * jnp.repeat(jnp.exp(draws), shape[dim] // shards_of).reshape((-1,) + (1,) * (len(shape) - 1 - dim))
    return gain


def normal_values(rng, shape, width, most, pieces=(), held_as=jnp.bfloat16):
    drawn = width * jax.random.normal(rng, shape, jnp.float32)
    if pieces:
        drawn = drawn * levels(rng, shape, pieces, -0.22, 0.18)
    return jnp.clip(drawn, -most, most).astype(held_as)


def setup_inputs(seed: int = 0) -> dict:
    key_of = jax.random.split(jax.random.key(seed), 10)
    mix_input = normal_values(key_of[0], (TOKENS_MIX, POOL), 1.0, 6.0, ((0, 32), (1, 16)))
    mix_weight = normal_values(key_of[1], (POOL, D), POOL ** -0.5, 0.125, ((1, 16),))
    expert_input = draw_expert_input(jax.random.fold_in(key_of[9], 71), 0)
    expert_index = draw_expert_index(jax.random.fold_in(key_of[9], 71), 0)
    route_share = jnp.clip(jnp.exp(math.log(1.0) - 2.3025851 * jax.random.uniform(key_of[4], (TOKENS_EXP, TOP), jnp.float32) ** levels(key_of[4], (TOKENS_EXP, TOP), ((0, 32),), -0.2, 0.2)), 0.1, 1.0)
    norm_gain = jnp.clip(1.0 + 0.18 * jax.random.normal(key_of[5], (D,), jnp.float32), 0.1, 1.9)
    gate_weight = normal_values(key_of[6], (EXPERTS, D, FF), D ** -0.5, 0.09375, ((0, 32), (2, 16)))
    up_weight = normal_values(key_of[7], (EXPERTS, D, FF), D ** -0.5, 0.09375, ((0, 32), (2, 16)))
    down_weight = normal_values(key_of[8], (EXPERTS, FF, D), FF ** -0.5, 0.125, ((0, 32), (2, 16)))
    return {"mix_input": mix_input, "mix_weight": mix_weight, "expert_input": expert_input, "expert_index": expert_index, "route_share": route_share, "norm_gain": norm_gain, "gate_weight": gate_weight, "up_weight": up_weight, "down_weight": down_weight}


window_reach = 15
norm_eps = 1e-06

def pool_minus_self(extended, first_pos, group_size, channel_base):
    length = extended.shape[0] - window_reach
    channels = extended.shape[1]
    channel = channel_base + jnp.arange(channels, dtype=jnp.int32)
    window = jnp.power(2, channel // group_size + 1).astype(jnp.int32)
    running = jnp.zeros((length, channels), jnp.float32)
    for lag_count in range(window_reach + 1):
        shifted = extended[window_reach - lag_count:window_reach - lag_count + length]
        running = running + jnp.where(lag_count < window[None, :], shifted, 0.0)
    position = first_pos + jnp.arange(length, dtype=jnp.int32)
    counts = jnp.minimum(position[:, None] + 1, window[None, :]).astype(jnp.float32)
    return (running / counts - extended[window_reach:]).astype(jnp.bfloat16)

def slot_targets(indices, experts, capacity):
    flattened = indices.reshape(-1)
    one_hot = (flattened[:, None] == jnp.arange(experts, dtype=jnp.int32)[None, :]).astype(jnp.int32)
    earlier = jnp.cumsum(one_hot, axis=0) - one_hot
    return flattened * capacity + lax.optimization_barrier(jnp.sum(earlier * one_hot, axis=1))

def reference(mix_input, mix_weight, expert_input, expert_index, route_share, norm_gain, gate_weight, up_weight, down_weight):
    extended = jnp.pad(mix_input.astype(jnp.float32), ((window_reach, 0), (0, 0)))
    pooled = pool_minus_self(extended, 0, POOL // 4, 0)
    mixed_rows = jnp.dot(pooled, mix_weight, preferred_element_type=jnp.float32).astype(jnp.bfloat16)
    blocks = expert_index.reshape(N_EP, TOK_EXP, TOP)
    targets = jax.vmap(partial(slot_targets, experts=EXPERTS, capacity=CAP))(blocks)
    expert_of = targets // CAP
    slot_of = targets % CAP
    source = jnp.arange(N_EP, dtype=jnp.int32)[:, None]
    placed = (expert_of * (N_EP * CAP) + source * CAP + slot_of).reshape(-1)
    row_ids = (source * TOK_EXP + jnp.repeat(jnp.arange(TOK_EXP, dtype=jnp.int32), TOP)[None, :]).reshape(-1)
    table = jnp.full((EXPERTS * N_EP * CAP,), TOKENS_EXP, jnp.int32).at[placed].set(row_ids)
    padded = jnp.concatenate([expert_input, jnp.zeros((1, D), jnp.bfloat16)], axis=0)

    def run_expert(operands):
        identity, gate_mat, up_mat, down_mat = operands
        rows_in = padded[identity]
        squares = lax.optimization_barrier(jnp.mean(jnp.square(rows_in.astype(jnp.float32)), axis=1, keepdims=True))
        inverse = lax.rsqrt(squares + norm_eps)
        scaled = (rows_in.astype(jnp.float32) * norm_gain).astype(jnp.bfloat16)
        gate_acts = jnp.dot(scaled, gate_mat, preferred_element_type=jnp.float32) * inverse
        up_acts = jnp.dot(scaled, up_mat, preferred_element_type=jnp.float32) * inverse
        hidden = (jax.nn.silu(gate_acts) * up_acts).astype(jnp.bfloat16)
        return jnp.dot(hidden, down_mat, preferred_element_type=jnp.float32).astype(jnp.bfloat16)
    produced = lax.map(run_expert, (table.reshape(EXPERTS, N_EP * CAP), gate_weight, up_weight, down_weight))
    picked = produced.reshape(EXPERTS * N_EP * CAP, D)[placed].astype(jnp.float32).reshape(TOKENS_EXP, TOP, D)
    shares = route_share / lax.optimization_barrier(jnp.sum(route_share, axis=1, keepdims=True))
    expert_rows = lax.optimization_barrier(jnp.sum(picked * shares[:, :, None], axis=1)).astype(jnp.bfloat16)
    return (mixed_rows, expert_rows)
```

```python
import functools

import jax
import jax.numpy as jnp
from jax import lax
from jax.experimental import pallas as pl
from jax.experimental.pallas import tpu as pltpu
from jax.sharding import PartitionSpec as P

MESH = pl.DeviceIdType.MESH
F32, BF16 = jnp.float32, jnp.bfloat16
norm_eps = 1e-06


def dot(a, b):
    return jnp.dot(a, b, preferred_element_type=F32)


def kernel(
    n_ep,
    n_x,
    n_tp,
    mix_in,
    mix_w,
    x_in,
    idx_in,
    share_in,
    gain_in,
    gate_w,
    up_w,
    down_w,
    mix_out,
    exp_out,
    X,
    H,
    M,
    W,
    D,
    MW,
    xin,
    mixin,
    halo,
    idx_v,
    share_v,
    gain_v,
    OUT,
    RET,
    Y,
    acc,
    sq,
    share_hi,
    share_lo,
    mixo,
    expo,
    ld_sem,
    st_sem,
    ring_send,
    ici,
    d2d,
    disp_send,
    disp_recv,
    ret_send,
    ret_recv,
    halo_sem,
):
    n_z = n_ep // n_x
    ny = n_tp // 2
    half_ring = ny // 2
    ep, t = lax.axis_index("ep"), lax.axis_index("tp")
    z, x = ep // n_x, ep % n_x
    y, core = t // 2, t % 2
    sibling = 2 * y + (1 - core)
    right = 2 * ((y + 1) % ny) + core
    left = 2 * ((y + ny - 1) % ny) + core
    cap = OUT.shape[0] // n_ep
    slots = OUT.shape[0]
    half = slots // 2
    tok = xin.shape[0]
    feat = xin.shape[1]
    ch = mixin.shape[1]
    mrows = mixo.shape[0]
    hid = H.shape[2]
    width = n_tp * feat

    def offset(k):
        i = k // n_x
        dz = jnp.where(i % 2 == 1, (i + 1) // 2, (n_z - i // 2) % n_z)
        return dz, k % n_x

    def source(k):
        dz, dx = offset(k)
        return ((z + dz) % n_z) * n_x + (x + dx) % n_x

    def target(k):
        dz, dx = offset(k)
        return ((z + n_z - dz) % n_z) * n_x + (x + n_x - dx) % n_x

    loads = [
        (idx_in, idx_v),
        (x_in, xin),
        (mix_in, mixin.at[pl.ds(16, mrows)]),
        (share_in, share_v),
        (gain_in, gain_v),
        (gate_w.at[0], W.at[:, pl.ds(0, hid)]),
        (up_w.at[0], W.at[:, pl.ds(hid, hid)]),
        (down_w.at[0], D),
        (mix_w, MW),
    ]
    loads = [pltpu.make_async_copy(a, b, ld_sem.at[i]) for i, (a, b) in enumerate(loads)]
    for copy in loads:
        copy.start()

    barrier = pltpu.get_barrier_semaphore()

    def greet(k, carry):
        pl.semaphore_signal(barrier, inc=1, device_id=(target(k), t), device_id_type=MESH)
        return carry

    for peer in (sibling, right, left):
        pl.semaphore_signal(barrier, inc=1, device_id=(ep, peer), device_id_type=MESH)
    lax.fori_loop(1, n_ep, greet, 0)

    loads[0].wait()
    first, second = idx_v[0:1, :], idx_v[1:2, :]
    experts = lax.broadcasted_iota(jnp.int32, (128, tok), 0)
    named = [(experts == row).astype(F32).astype(BF16) for row in (first, second)]
    before = lax.broadcasted_iota(jnp.int32, (tok, tok), 0) < lax.broadcasted_iota(
        jnp.int32, (tok, tok), 1
    )
    both = named[0] + named[1]
    counts = dot(both, before.astype(F32).astype(BF16)).astype(BF16)
    slot = lax.broadcasted_iota(jnp.int32, (slots, 128), 0)
    owner = lax.broadcasted_iota(jnp.int32, (slots, 128), 1)
    spread = (slot // cap == owner).astype(F32).astype(BF16)
    place = (lax.broadcasted_iota(jnp.int32, (slots, tok), 0) % cap).astype(F32)
    hit = dot(spread, counts) == place
    picks = [
        jnp.where(jnp.logical_and(hit, dot(spread, row) > 0.5), 1.0, 0.0) for row in named
    ]
    loads[1].wait()
    OUT[...] = dot((picks[0] + picks[1]).astype(BF16), xin[...]).astype(BF16)

    loads[2].wait()
    window = lax.shift_left(jnp.int32(2), t // (n_tp // 4))

    def pooled(ext, first_pos):
        total = ext
        for step in (1, 2, 4, 8):
            shifted = pltpu.roll(total, step, 0)
            total = jnp.where(window > step, total + shifted, total)
        rows = ext.shape[0]
        pos = lax.broadcasted_iota(jnp.int32, (rows, ch), 0) + (first_pos - 16)
        div = jnp.minimum(jnp.maximum(pos + 1, 1), window).astype(F32)
        return (total / div - ext)[16:].astype(BF16)

    mixin[0:16, :] = jnp.zeros((16, ch), BF16)
    M[t] = pooled(mixin[...].astype(F32), ep * mrows)
    acc[...] = jnp.zeros(acc.shape, F32)
    sq[...] = jnp.zeros(sq.shape, F32)

    pl.semaphore_wait(barrier, n_ep + 2)

    halo_copy = pltpu.make_async_remote_copy(
        src_ref=mixin.at[pl.ds(mrows, 16)],
        dst_ref=halo,
        send_sem=halo_sem.at[0],
        recv_sem=halo_sem.at[1],
        device_id=((ep + 1) % n_ep, t),
        device_id_type=MESH,
    )
    halo_copy.start()

    def ring(rid, buf, base, rows, nq):
        cr = rows // nq

        def chunk(block, q):
            return buf.at[block, pl.ds(base + q * cr, cr)]

        def push(block, q, peer, recv):
            pltpu.make_async_remote_copy(
                src_ref=chunk(block, q),
                dst_ref=chunk(block, q),
                send_sem=ring_send.at[rid],
                recv_sem=recv,
                device_id=(ep, peer),
                device_id_type=MESH,
            ).start()

        def arrived(block, q, recv):
            pltpu.make_async_remote_copy(
                src_ref=chunk(block, q),
                dst_ref=chunk(block, q),
                send_sem=ring_send.at[rid],
                recv_sem=recv,
                device_id=(ep, sibling),
                device_id_type=MESH,
            ).wait_recv()

        def begin(qs):
            for q in qs:
                if half_ring > 1 or q % 2 == 0:
                    push(t, q, right, ici.at[rid, 1, q])
                if half_ring > 1 or q % 2 == 1:
                    push(t, q, left, ici.at[rid, ny - 1, q])
            for q in qs:
                push(t, q, sibling, d2d.at[rid, 0, q])

        def step(s):
            for q in range(nq):
                if s < half_ring or q % 2 == 0:
                    block = 2 * ((y + ny - s) % ny) + core
                    arrived(block, q, ici.at[rid, s, q])
                    if s + 1 < half_ring or (s + 1 == half_ring and q % 2 == 0):
                        push(block, q, right, ici.at[rid, s + 1, q])
                    push(block, q, sibling, d2d.at[rid, s, q])
                if s < half_ring or q % 2 == 1:
                    block = 2 * ((y + s) % ny) + core
                    arrived(block, q, ici.at[rid, ny - s, q])
                    if s + 1 < half_ring or (s + 1 == half_ring and q % 2 == 1):
                        push(block, q, left, ici.at[rid, ny - s - 1, q])
                    push(block, q, sibling, d2d.at[rid, ny - s, q])

        def from_sibling(rel):
            block = 2 * ((y + ny - rel) % ny) + (1 - core)
            for q in range(nq):
                arrived(block, q, d2d.at[rid, rel, q])

        def drain():
            whole = buf.at[pl.ds(0, n_tp - 1), pl.ds(base, rows)]
            pltpu.make_async_remote_copy(
                src_ref=whole,
                dst_ref=whole,
                send_sem=ring_send.at[rid],
                recv_sem=ici.at[rid, 1, 0],
                device_id=(ep, sibling),
                device_id_type=MESH,
            ).wait_send()

        return begin, step, from_sibling, drain

    nqm, nqx, nqh = 4, 2, 2
    m_ring = ring(0, M, 0, mrows, nqm)
    x_rings = [ring(1 + h, X, h * half, half, nqx) for h in (0, 1)]
    h_rings = [ring(3 + h, H, h * half, half, nqh) for h in (0, 1)]

    m_ring[0](range(1, nqm))

    def dispatch(h):
        def send(k, carry):
            to = target(k)
            pltpu.make_async_remote_copy(
                src_ref=OUT.at[pl.ds(pl.multiple_of(to * cap, cap), cap)],
                dst_ref=X.at[t, pl.ds(pl.multiple_of(k * cap, cap), cap)],
                send_sem=disp_send,
                recv_sem=disp_recv.at[h],
                device_id=(to, t),
                device_id_type=MESH,
            ).start()
            return carry

        lax.fori_loop(max(1, h * (n_ep // 2)), (h + 1) * (n_ep // 2), send, 0)

    dispatch(0)
    dispatch(1)
    X[t, pl.ds(0, cap)] = OUT[pl.ds(pl.multiple_of(ep * cap, cap), cap)]

    def dispatched(h):
        rows = X.at[t, pl.ds(cap, half - cap)] if h == 0 else X.at[t, pl.ds(half, half)]
        pltpu.make_async_remote_copy(
            src_ref=rows,
            dst_ref=rows,
            send_sem=disp_send,
            recv_sem=disp_recv.at[h],
            device_id=(ep, sibling),
            device_id_type=MESH,
        ).wait_recv()

    halo_copy.wait_recv()
    past = jnp.where(ep > 0, halo[...].astype(F32), 0.0)
    head = jnp.concatenate([past, mixin[16:32, :].astype(F32)], axis=0)
    M[t, 0:16] = pooled(head, ep * mrows)
    m_ring[0](range(0, 1))

    loads[3].wait()
    s0, s1 = share_v[0:1, :], share_v[1:2, :]
    total = s0 + s1
    weights = picks[0] * (s0 / total) + picks[1] * (s1 / total)
    high = weights.astype(BF16)
    share_hi[...] = high.astype(F32).T.astype(BF16)
    share_lo[...] = (weights - high.astype(F32)).T.astype(BF16)

    m_ring[1](1)
    for copy in loads[4:]:
        copy.wait()

    tile = min(128, half)

    def gather_unit(h, rel):
        x_rings[h][2](rel)
        chip = (y + ny - rel) % ny
        cols = pl.ds(pl.multiple_of(chip * 2 * feat, 2 * feat), 2 * feat)

        def body(i, carry):
            rows = pl.ds(pl.multiple_of(h * half + i * tile, tile), tile)
            value = jnp.concatenate([X[2 * chip, rows], X[2 * chip + 1, rows]], axis=1)
            value = value.astype(F32)
            scaled = (value * gain_v[:, cols]).astype(BF16)
            acc[rows, :] += dot(scaled, W[cols, :])
            square = value * value
            part = square[:, 0:128]
            for j in range(1, 2 * feat // 128):
                part += square[:, j * 128 : (j + 1) * 128]
            sq[rows, :] += part
            return carry

        lax.fori_loop(0, half // tile, body, 0)

    def gather_half(h, then):
        for s in range(1, half_ring):
            x_rings[h][1](s)
            if s == half_ring - 1:
                then()
            if s == 1:
                gather_unit(h, 0)
            else:
                gather_unit(h, s - 1)
                gather_unit(h, ny - s + 1)
        x_rings[h][1](half_ring)
        gather_unit(h, half_ring - 1)
        gather_unit(h, ny - half_ring + 1)
        gather_unit(h, half_ring)

    def activate(h):
        def body(i, carry):
            rows = pl.ds(pl.multiple_of(h * half + i * tile, tile), tile)
            inverse = lax.rsqrt(jnp.sum(sq[rows, :], axis=1, keepdims=True) / width + norm_eps)
            gate = acc[rows, 0:hid] * inverse
            up = acc[rows, hid : 2 * hid] * inverse
            H[t, rows] = (gate / (1.0 + jnp.exp(-gate)) * up).astype(BF16)
            return carry

        lax.fori_loop(0, half // tile, body, 0)

    def project(blocks, rows, weight):
        total = None
        for i in range(0, n_tp, 2):
            value = jnp.concatenate([blocks[i, rows], blocks[i + 1, rows]], axis=1)
            depth = value.shape[1]
            term = dot(value, weight[(i // 2) * depth : (i // 2 + 1) * depth, :])
            total = term if total is None else total + term
        return total.astype(BF16)

    def hidden_half(h, then):
        for s in range(1, half_ring):
            h_rings[h][1](s)
            if s == half_ring - 1:
                then()
        h_rings[h][1](half_ring)
        for rel in range(ny):
            h_rings[h][2](rel)

        def body(i, carry):
            rows = pl.ds(pl.multiple_of(h * half + i * tile, tile), tile)
            Y[rows, :] = project(H, rows, D)
            return carry

        lax.fori_loop(0, half // tile, body, 0)

        def send(k, carry):
            pltpu.make_async_remote_copy(
                src_ref=Y.at[pl.ds(pl.multiple_of(k * cap, cap), cap)],
                dst_ref=RET.at[pl.ds(pl.multiple_of(ep * cap, cap), cap)],
                send_sem=ret_send,
                recv_sem=ret_recv,
                device_id=(source(k), t),
                device_id_type=MESH,
            ).start()
            return carry

        lax.fori_loop(max(1, h * (n_ep // 2)), (h + 1) * (n_ep // 2), send, 0)

    def start_far():
        dispatched(1)
        x_rings[1][0](range(nqx))

    def start_hidden_near():
        activate(0)
        h_rings[0][0](range(nqh))

    def start_hidden_far():
        pass

    dispatched(0)
    x_rings[0][0](range(nqx))
    gather_half(0, start_far)
    gather_half(1, start_hidden_near)
    activate(1)
    h_rings[1][0](range(nqh))
    hidden_half(0, start_hidden_far)
    hidden_half(1, start_hidden_far)

    for s in range(2, half_ring + 1):
        m_ring[1](s)
    for rel in range(ny):
        m_ring[2](rel)

    def mix_tile(i, carry):
        rows = pl.ds(pl.multiple_of(i * 128, 128), 128)
        mixo[rows, :] = project(M, rows, MW)
        return carry

    lax.fori_loop(0, mrows // 128, mix_tile, 0)
    mix_store = pltpu.make_async_copy(mixo, mix_out, st_sem.at[0])
    mix_store.start()

    RET[pl.ds(pl.multiple_of(ep * cap, cap), cap)] = Y[0:cap]
    back = RET.at[pl.ds(0, slots - cap)]
    pltpu.make_async_remote_copy(
        src_ref=back,
        dst_ref=back,
        send_sem=ret_send,
        recv_sem=ret_recv,
        device_id=(ep, sibling),
        device_id_type=MESH,
    ).wait_recv()
    expo[...] = (dot(share_hi[...], RET[...]) + dot(share_lo[...], RET[...])).astype(BF16)
    exp_store = pltpu.make_async_copy(expo, exp_out, st_sem.at[1])
    exp_store.start()

    halo_copy.wait_send()
    for r in [m_ring, *x_rings, *h_rings]:
        r[3]()
    for buf, sem in ((OUT, disp_send), (Y, ret_send)):
        rows = buf.at[pl.ds(0, slots - cap)]
        pltpu.make_async_remote_copy(
            src_ref=rows,
            dst_ref=rows,
            send_sem=sem,
            recv_sem=ret_recv,
            device_id=(ep, sibling),
            device_id_type=MESH,
        ).wait_send()
    mix_store.wait()
    exp_store.wait()


def shards(
    n_ep,
    n_tp,
    mix_input,
    mix_weight,
    expert_input,
    expert_index,
    route_share,
    norm_gain,
    gate_weight,
    up_weight,
    down_weight,
):
    mrows, ch = mix_input.shape
    cols = mix_weight.shape[1]
    tok, feat = expert_input.shape
    hid = gate_weight.shape[2]
    out_feat = down_weight.shape[2]
    width = norm_gain.shape[0]
    n_x = 4 if n_ep % 4 == 0 else 1
    slots = 2 * tok * expert_index.shape[1]
    ny = n_tp // 2
    dma = pltpu.SemaphoreType.DMA
    anywhere = pl.BlockSpec(memory_space=pl.ANY)
    return pl.pallas_call(
        functools.partial(kernel, n_ep, n_x, n_tp),
        out_shape=(
            jax.ShapeDtypeStruct((mrows, cols), BF16),
            jax.ShapeDtypeStruct((tok, out_feat), BF16),
        ),
        in_specs=[anywhere] * 9,
        out_specs=(anywhere, anywhere),
        scratch_shapes=[
            pltpu.VMEM((n_tp, slots, feat), BF16),
            pltpu.VMEM((n_tp, slots, hid), BF16),
            pltpu.VMEM((n_tp, mrows, ch), BF16),
            pltpu.VMEM((width, 2 * hid), BF16),
            pltpu.VMEM((n_tp * hid, out_feat), BF16),
            pltpu.VMEM((n_tp * ch, cols), BF16),
            pltpu.VMEM((tok, feat), BF16),
            pltpu.VMEM((mrows + 16, ch), BF16),
            pltpu.VMEM((16, ch), BF16),
            pltpu.VMEM((2, tok), jnp.int32),
            pltpu.VMEM((2, tok), F32),
            pltpu.VMEM((1, width), F32),
            pltpu.VMEM((slots, feat), BF16),
            pltpu.VMEM((slots, out_feat), BF16),
            pltpu.VMEM((slots, out_feat), BF16),
            pltpu.VMEM((slots, 2 * hid), F32),
            pltpu.VMEM((slots, 128), F32),
            pltpu.VMEM((tok, slots), BF16),
            pltpu.VMEM((tok, slots), BF16),
            pltpu.VMEM((mrows, cols), BF16),
            pltpu.VMEM((tok, out_feat), BF16),
            dma((9,)),
            dma((2,)),
            dma((5,)),
            dma((5, ny, 4)),
            dma((5, ny, 4)),
            dma,
            dma((2,)),
            dma,
            dma,
            dma((2,)),
        ],
        compiler_params=pltpu.CompilerParams(
            collective_id=0, has_side_effects=True, vmem_limit_bytes=48 * 2**20
        ),
    )(
        mix_input,
        mix_weight,
        expert_input,
        expert_index.T,
        route_share.T,
        norm_gain.reshape(1, width),
        gate_weight,
        up_weight,
        down_weight,
    )


def solution(mesh):
    placed = (
        P("ep", "tp"),
        P(None, "tp"),
        P("ep", "tp"),
        P("ep", None),
        P("ep", None),
        P(),
        P("ep", None, "tp"),
        P("ep", None, "tp"),
        P("ep", None, "tp"),
    )
    return jax.shard_map(
        functools.partial(shards, mesh.shape["ep"], mesh.shape["tp"]),
        mesh=mesh,
        in_specs=placed,
        out_specs=(P("ep", "tp"), P("ep", "tp")),
        check_vma=False,
    )
```

```python
import functools

import jax
import jax.numpy as jnp
from jax import lax
from jax.experimental import pallas as pl
from jax.experimental.pallas import tpu as pltpu
from jax.sharding import PartitionSpec as P

MESH = pl.DeviceIdType.MESH
F32, BF16 = jnp.float32, jnp.bfloat16
norm_eps = 1e-06


def dot(a, b):
    return jnp.dot(a, b, preferred_element_type=F32)


def kernel(
    n_ep,
    n_x,
    n_tp,
    mix_in,
    mix_w,
    x_in,
    idx_in,
    share_in,
    gain_in,
    gate_w,
    up_w,
    down_w,
    mix_out,
    exp_out,
    X,
    H,
    M,
    W,
    D,
    MW,
    xin,
    mixin,
    halo,
    idx_v,
    share_v,
    gain_v,
    OUT,
    RET,
    Y,
    acc,
    sq,
    share_hi,
    share_lo,
    mixo,
    expo,
    ld_sem,
    st_sem,
    ring_send,
    ici,
    d2d,
    disp_send,
    disp_recv,
    ret_send,
    ret_recv,
    halo_sem,
):
    n_z = n_ep // n_x
    ny = n_tp // 2
    half_ring = ny // 2
    ep, t = lax.axis_index("ep"), lax.axis_index("tp")
    z, x = ep // n_x, ep % n_x
    y, core = t // 2, t % 2
    sibling = 2 * y + (1 - core)
    right = 2 * ((y + 1) % ny) + core
    left = 2 * ((y + ny - 1) % ny) + core
    cap = OUT.shape[0] // n_ep
    slots = OUT.shape[0]
    half = slots // 2
    tok = xin.shape[0]
    feat = xin.shape[1]
    ch = mixin.shape[1]
    mrows = mixo.shape[0]
    hid = H.shape[2]
    width = n_tp * feat

    def offset(k):
        i = k // n_x
        return ((i + 1) // 2 if i % 2 else (n_z - i // 2) % n_z), k % n_x

    def source(k):
        dz, dx = offset(k)
        return lax.rem(z + dz, n_z) * n_x + lax.rem(x + dx, n_x)

    def target(k):
        dz, dx = offset(k)
        return lax.rem(z + n_z - dz, n_z) * n_x + lax.rem(x + n_x - dx, n_x)

    loads = [
        (idx_in, idx_v),
        (x_in, xin),
        (mix_in, mixin.at[pl.ds(16, mrows)]),
        (share_in, share_v),
        (gain_in, gain_v),
        (gate_w.at[0], W.at[:, pl.ds(0, hid)]),
        (up_w.at[0], W.at[:, pl.ds(hid, hid)]),
        (down_w.at[0], D),
        (mix_w, MW),
    ]
    loads = [pltpu.make_async_copy(a, b, ld_sem.at[i]) for i, (a, b) in enumerate(loads)]
    for copy in loads:
        copy.start()

    barrier = pltpu.get_barrier_semaphore()

    for k in range(n_ep - 1, 0, -1):
        pl.semaphore_signal(barrier, inc=1, device_id=(target(k), t), device_id_type=MESH)
    for peer in (sibling, right, left):
        pl.semaphore_signal(barrier, inc=1, device_id=(ep, peer), device_id_type=MESH)

    with jax.named_scope("l0"):
        loads[0].wait()
    first, second = idx_v[0:1, :], idx_v[1:2, :]
    experts = lax.broadcasted_iota(jnp.int32, (128, tok), 0)
    named = [(experts == row).astype(F32).astype(BF16) for row in (first, second)]
    before = lax.broadcasted_iota(jnp.int32, (tok, tok), 0) < lax.broadcasted_iota(
        jnp.int32, (tok, tok), 1
    )
    both = named[0] + named[1]
    counts = dot(both, before.astype(F32).astype(BF16)).astype(BF16)
    slot = lax.broadcasted_iota(jnp.int32, (slots, 128), 0)
    owner = lax.broadcasted_iota(jnp.int32, (slots, 128), 1)
    spread = (slot // cap == owner).astype(F32).astype(BF16)
    place = (lax.broadcasted_iota(jnp.int32, (slots, tok), 0) % cap).astype(F32)
    hit = dot(spread, counts) == place
    picks = [
        jnp.where(jnp.logical_and(hit, dot(spread, row) > 0.5), 1.0, 0.0) for row in named
    ]
    with jax.named_scope("l1"):
        loads[1].wait()
    OUT[...] = dot((picks[0] + picks[1]).astype(BF16), xin[...]).astype(BF16)

    with jax.named_scope("l2"):
        loads[2].wait()
    window = lax.shift_left(jnp.int32(2), t // (n_tp // 4))

    def pooled(ext, first_pos):
        total = ext
        for step in (1, 2, 4, 8):
            shifted = pltpu.roll(total, step, 0)
            total = jnp.where(window > step, total + shifted, total)
        rows = ext.shape[0]
        pos = lax.broadcasted_iota(jnp.int32, (rows, ch), 0) + (first_pos - 16)
        div = jnp.minimum(jnp.maximum(pos + 1, 1), window).astype(F32)
        return (total / div - ext)[16:].astype(BF16)

    mixin[0:16, :] = jnp.zeros((16, ch), BF16)
    M[t] = pooled(mixin[...].astype(F32), ep * mrows)
    acc[...] = jnp.zeros(acc.shape, F32)
    sq[...] = jnp.zeros(sq.shape, F32)

    with jax.named_scope("bar"):
        pl.semaphore_wait(barrier, n_ep + 2)

    halo_copy = pltpu.make_async_remote_copy(
        src_ref=mixin.at[pl.ds(mrows, 16)],
        dst_ref=halo,
        send_sem=halo_sem.at[0],
        recv_sem=halo_sem.at[1],
        device_id=((ep + 1) % n_ep, t),
        device_id_type=MESH,
    )
    halo_copy.start()

    def ring(rid, buf, rows, nq):
        cr = rows // nq

        def chunk(block, q):
            return buf.at[block, pl.ds(q * cr, cr)]

        def push(block, q, peer, recv):
            pltpu.make_async_remote_copy(
                src_ref=chunk(block, q),
                dst_ref=chunk(block, q),
                send_sem=ring_send.at[rid],
                recv_sem=recv,
                device_id=(ep, peer),
                device_id_type=MESH,
            ).start()

        def arrived(block, q, recv):
            pltpu.make_async_remote_copy(
                src_ref=chunk(block, q),
                dst_ref=chunk(block, q),
                send_sem=ring_send.at[rid],
                recv_sem=recv,
                device_id=(ep, sibling),
                device_id_type=MESH,
            ).wait_recv()

        def begin(q):
            push(t, q, right, ici.at[rid, 1, q])
            push(t, q, left, ici.at[rid, ny - 1, q])
            push(t, q, sibling, d2d.at[rid, 0, q])

        def step(s, q):
            if s < half_ring or q % 2 == 0:
                block = 2 * lax.rem(y + ny - s, ny) + core
                arrived(block, q, ici.at[rid, s, q])
                if s + 1 < half_ring or (s + 1 == half_ring and q % 2 == 0):
                    push(block, q, right, ici.at[rid, s + 1, q])
                push(block, q, sibling, d2d.at[rid, s, q])
            if s < half_ring or q % 2 == 1:
                block = 2 * lax.rem(y + s, ny) + core
                arrived(block, q, ici.at[rid, ny - s, q])
                if s + 1 < half_ring or (s + 1 == half_ring and q % 2 == 1):
                    push(block, q, left, ici.at[rid, ny - s - 1, q])
                push(block, q, sibling, d2d.at[rid, ny - s, q])

        def from_sibling(rel, q):
            block = 2 * lax.rem(y + ny - rel, ny) + (1 - core)
            arrived(block, q, d2d.at[rid, rel, q])

        def drain():
            whole = buf.at[pl.ds(0, n_tp - 1)]
            pltpu.make_async_remote_copy(
                src_ref=whole,
                dst_ref=whole,
                send_sem=ring_send.at[rid],
                recv_sem=ici.at[rid, 1, 0],
                device_id=(ep, sibling),
                device_id_type=MESH,
            ).wait_send()

        return begin, step, from_sibling, drain

    nq = 4
    m_ring = ring(0, M, mrows, nq)
    x_ring = ring(1, X, slots, nq)
    h_ring = ring(2, H, slots, nq)

    def dispatch(h):
        for k in range(max(1, h * (n_ep // 2)), (h + 1) * (n_ep // 2)):
            to = target(k)
            pltpu.make_async_remote_copy(
                src_ref=OUT.at[pl.ds(pl.multiple_of(to * cap, cap), cap)],
                dst_ref=X.at[t, pl.ds(k * cap, cap)],
                send_sem=disp_send,
                recv_sem=disp_recv.at[h],
                device_id=(to, t),
                device_id_type=MESH,
            ).start()

    with jax.named_scope("dispatch"):
        dispatch(0)
        dispatch(1)
    for q in range(1, nq):
        m_ring[0](q)
    X[t, pl.ds(0, cap)] = OUT[pl.ds(pl.multiple_of(ep * cap, cap), cap)]

    def dispatched(h):
        rows = X.at[t, pl.ds(cap, half - cap)] if h == 0 else X.at[t, pl.ds(half, half)]
        pltpu.make_async_remote_copy(
            src_ref=rows,
            dst_ref=rows,
            send_sem=disp_send,
            recv_sem=disp_recv.at[h],
            device_id=(ep, sibling),
            device_id_type=MESH,
        ).wait_recv()

    loads[3].wait()
    s0, s1 = share_v[0:1, :], share_v[1:2, :]
    total = s0 + s1
    weights = picks[0] * (s0 / total) + picks[1] * (s1 / total)
    high = weights.astype(BF16)
    share_hi[...] = high.astype(F32).T.astype(BF16)
    share_lo[...] = (weights - high.astype(F32)).T.astype(BF16)

    with jax.named_scope("halo"):
        halo_copy.wait_recv()
    past = jnp.where(ep > 0, halo[...].astype(F32), 0.0)
    head = jnp.concatenate([past, mixin[16:32, :].astype(F32)], axis=0)
    M[t, 0:16] = pooled(head, ep * mrows)
    m_ring[0](0)

    with jax.named_scope("m1"):
        for q in range(1, nq):
            m_ring[1](1, q)
    with jax.named_scope("disp0"):
        dispatched(0)
    for q in range(nq // 2):
        x_ring[0](q)
    with jax.named_scope("m10"):
        m_ring[1](1, 0)
    with jax.named_scope("disp1"):
        dispatched(1)
    for q in range(nq // 2, nq):
        x_ring[0](q)
    for copy in loads[4:]:
        copy.wait()

    tile = slots // nq

    def gather_tile(rel, q):
        x_ring[2](rel, q)
        chip = lax.rem(y + ny - rel, ny)
        cols = pl.ds(pl.multiple_of(chip * 2 * feat, 2 * feat), 2 * feat)
        rows = pl.ds(q * tile, tile)
        value = jnp.concatenate([X[2 * chip, rows], X[2 * chip + 1, rows]], axis=1)
        value = value.astype(F32)
        scaled = (value * gain_v[:, cols]).astype(BF16)
        acc[rows, :] += dot(scaled, W[cols, :])
        square = value * value
        part = square[:, 0:128]
        for j in range(1, 2 * feat // 128):
            part += square[:, j * 128 : (j + 1) * 128]
        sq[rows, :] += part

    def activate(q):
        rows = pl.ds(q * tile, tile)
        inverse = lax.rsqrt(jnp.sum(sq[rows, :], axis=1, keepdims=True) / width + norm_eps)
        gate = acc[rows, 0:hid] * inverse
        up = acc[rows, hid : 2 * hid] * inverse
        H[t, rows] = (gate / (1.0 + jnp.exp(-gate)) * up).astype(BF16)
        acc[rows, :] = jnp.zeros((tile, 2 * hid), F32)

    def down_tile(rel, q):
        h_ring[2](rel, q)
        chip = lax.rem(y + ny - rel, ny)
        cols = pl.ds(pl.multiple_of(chip * 2 * hid, 2 * hid), 2 * hid)
        rows = pl.ds(q * tile, tile)
        value = jnp.concatenate([H[2 * chip, rows], H[2 * chip + 1, rows]], axis=1)
        acc[rows, :] += dot(value, D[cols, :])

    def project(blocks, rows, weight):
        total = None
        for i in range(0, n_tp, 2):
            value = jnp.concatenate([blocks[i, rows], blocks[i + 1, rows]], axis=1)
            depth = value.shape[1]
            term = dot(value, weight[(i // 2) * depth : (i // 2 + 1) * depth, :])
            total = term if total is None else total + term
        return total.astype(BF16)

    def tiles_at(tile_of, distance, q):
        tile_of(distance, q)
        if distance > 0:
            tile_of(ny - distance, q)

    def travel(name, ring, tile_of, woven, between, finish):
        for s in range(1, half_ring):
            with jax.named_scope(f"{name}{s}"):
                if woven:
                    for q in range(nq):
                        ring[1](s, q)
                        tiles_at(tile_of, s - 1, q)
                else:
                    for q in range(nq):
                        ring[1](s, q)
                    for q in range(nq):
                        tiles_at(tile_of, s - 1, q)
        with jax.named_scope(f"{name}b"):
            between()
            for q in range(nq):
                tiles_at(tile_of, half_ring - 1, q)
        with jax.named_scope(f"{name}{half_ring}"):
            for q in range(nq):
                ring[1](half_ring, q)
        with jax.named_scope(f"{name}end"):
            for q in range(nq):
                tile_of(half_ring, q)
                finish(q)

    def begin_hidden(q):
        activate(q)
        h_ring[0](q)

    def mixer(s):
        for q in (*range(1, nq), 0):
            m_ring[1](s, q)

    def give_back(q):
        rows = pl.ds(q * tile, tile)
        Y[rows, :] = acc[rows, :].astype(BF16)
        per = n_ep // nq
        for k in range(max(1, q * per), (q + 1) * per):
            pltpu.make_async_remote_copy(
                src_ref=Y.at[pl.ds(k * cap, cap)],
                dst_ref=RET.at[pl.ds(pl.multiple_of(ep * cap, cap), cap)],
                send_sem=ret_send,
                recv_sem=ret_recv,
                device_id=(source(k), t),
                device_id_type=MESH,
            ).start()

    travel("x", x_ring, gather_tile, True, lambda: None, begin_hidden)
    travel("h", h_ring, down_tile, False, lambda: mixer(2), give_back)
    with jax.named_scope("mrest"):
        for s in range(3, half_ring + 1):
            mixer(s)

    for rel in range(ny):
        for q in range(nq):
            m_ring[2](rel, q)

    def mix_tile(i, carry):
        rows = pl.ds(pl.multiple_of(i * 128, 128), 128)
        mixo[rows, :] = project(M, rows, MW)
        return carry

    with jax.named_scope("mixdot"):
        lax.fori_loop(0, mrows // 128, mix_tile, 0)
    mix_store = pltpu.make_async_copy(mixo, mix_out, st_sem.at[0])
    mix_store.start()

    RET[pl.ds(pl.multiple_of(ep * cap, cap), cap)] = Y[0:cap]
    back = RET.at[pl.ds(0, slots - cap)]
    with jax.named_scope("retwait"):
        pltpu.make_async_remote_copy(
            src_ref=back,
            dst_ref=back,
            send_sem=ret_send,
            recv_sem=ret_recv,
            device_id=(ep, sibling),
            device_id_type=MESH,
        ).wait_recv()
    with jax.named_scope("combine"):
        expo[...] = (dot(share_hi[...], RET[...]) + dot(share_lo[...], RET[...])).astype(BF16)
    exp_store = pltpu.make_async_copy(expo, exp_out, st_sem.at[1])
    exp_store.start()

    with jax.named_scope("drain"):
        halo_copy.wait_send()
        for r in (m_ring, x_ring, h_ring):
            r[3]()
        for buf, sem in ((OUT, disp_send), (Y, ret_send)):
            rows = buf.at[pl.ds(0, slots - cap)]
            pltpu.make_async_remote_copy(
                src_ref=rows,
                dst_ref=rows,
                send_sem=sem,
                recv_sem=ret_recv,
                device_id=(ep, sibling),
                device_id_type=MESH,
            ).wait_send()
        mix_store.wait()
        exp_store.wait()


def shards(
    n_ep,
    n_tp,
    mix_input,
    mix_weight,
    expert_input,
    expert_index,
    route_share,
    norm_gain,
    gate_weight,
    up_weight,
    down_weight,
):
    mrows, ch = mix_input.shape
    cols = mix_weight.shape[1]
    tok, feat = expert_input.shape
    hid = gate_weight.shape[2]
    out_feat = down_weight.shape[2]
    width = norm_gain.shape[0]
    n_x = 4 if n_ep % 4 == 0 else 1
    slots = 2 * tok * expert_index.shape[1]
    ny = n_tp // 2
    dma = pltpu.SemaphoreType.DMA
    anywhere = pl.BlockSpec(memory_space=pl.ANY)
    return pl.pallas_call(
        functools.partial(kernel, n_ep, n_x, n_tp),
        out_shape=(
            jax.ShapeDtypeStruct((mrows, cols), BF16),
            jax.ShapeDtypeStruct((tok, out_feat), BF16),
        ),
        in_specs=[anywhere] * 9,
        out_specs=(anywhere, anywhere),
        scratch_shapes=[
            pltpu.VMEM((n_tp, slots, feat), BF16),
            pltpu.VMEM((n_tp, slots, hid), BF16),
            pltpu.VMEM((n_tp, mrows, ch), BF16),
            pltpu.VMEM((width, 2 * hid), BF16),
            pltpu.VMEM((n_tp * hid, out_feat), BF16),
            pltpu.VMEM((n_tp * ch, cols), BF16),
            pltpu.VMEM((tok, feat), BF16),
            pltpu.VMEM((mrows + 16, ch), BF16),
            pltpu.VMEM((16, ch), BF16),
            pltpu.VMEM((2, tok), jnp.int32),
            pltpu.VMEM((2, tok), F32),
            pltpu.VMEM((1, width), F32),
            pltpu.VMEM((slots, feat), BF16),
            pltpu.VMEM((slots, out_feat), BF16),
            pltpu.VMEM((slots, out_feat), BF16),
            pltpu.VMEM((slots, 2 * hid), F32),
            pltpu.VMEM((slots, 128), F32),
            pltpu.VMEM((tok, slots), BF16),
            pltpu.VMEM((tok, slots), BF16),
            pltpu.VMEM((mrows, cols), BF16),
            pltpu.VMEM((tok, out_feat), BF16),
            dma((9,)),
            dma((2,)),
            dma((3,)),
            dma((3, ny, 4)),
            dma((3, ny, 4)),
            dma,
            dma((2,)),
            dma,
            dma,
            dma((2,)),
        ],
        compiler_params=pltpu.CompilerParams(
            collective_id=0, has_side_effects=True, vmem_limit_bytes=67043328
        ),
    )(
        mix_input,
        mix_weight,
        expert_input,
        expert_index.T,
        route_share.T,
        norm_gain.reshape(1, width),
        gate_weight,
        up_weight,
        down_weight,
    )


def solution(mesh):
    placed = (
        P("ep", "tp"),
        P(None, "tp"),
        P("ep", "tp"),
        P("ep", None),
        P("ep", None),
        P(),
        P("ep", None, "tp"),
        P("ep", None, "tp"),
        P("ep", None, "tp"),
    )
    return jax.shard_map(
        functools.partial(shards, mesh.shape["ep"], mesh.shape["tp"]),
        mesh=mesh,
        in_specs=placed,
        out_specs=(P("ep", "tp"), P("ep", "tp")),
        check_vma=False,
    )
```

```python
import functools

import jax
import jax.numpy as jnp
from jax import lax
from jax.experimental import pallas as pl
from jax.experimental.pallas import tpu as pltpu
from jax.sharding import PartitionSpec as P

MESH = pl.DeviceIdType.MESH
F32, BF16 = jnp.float32, jnp.bfloat16
norm_eps = 1e-06


def dot(a, b):
    return jnp.dot(a, b, preferred_element_type=F32)


def kernel(
    n_ep,
    n_x,
    n_tp,
    mix_in,
    mix_w,
    x_in,
    idx_in,
    share_in,
    gain_in,
    gate_w,
    up_w,
    down_w,
    mix_out,
    exp_out,
    X,
    H,
    M,
    W,
    D,
    MW,
    xin,
    mixin,
    halo,
    idx_v,
    share_v,
    gain_v,
    OUT,
    RET,
    Y,
    acc,
    sq,
    share_hi,
    share_lo,
    ld_sem,
    ring_send,
    ici,
    d2d,
    m_ici,
    m_d2d,
    disp_send,
    disp_recv,
    ret_send,
    ret_recv,
    halo_sem,
):
    n_z = n_ep // n_x
    ny = n_tp // 2
    half_ring = ny // 2
    ep, t = lax.axis_index("ep"), lax.axis_index("tp")
    z, x = ep // n_x, ep % n_x
    y, core = t // 2, t % 2
    sibling = 2 * y + (1 - core)
    right = 2 * ((y + 1) % ny) + core
    left = 2 * ((y + ny - 1) % ny) + core
    right2 = 2 * ((y + 2) % ny) + core
    left2 = 2 * ((y + ny - 2) % ny) + core
    cap = OUT.shape[0] // n_ep
    slots = OUT.shape[0]
    half = slots // 2
    tok = xin.shape[0]
    feat = xin.shape[1]
    ch = mixin.shape[1]
    mrows = mix_out.shape[0]
    hid = H.shape[2]
    width = n_tp * feat

    def offset(k):
        i = k // n_x
        return ((i + 1) // 2 if i % 2 else (n_z - i // 2) % n_z), k % n_x

    def source(k):
        dz, dx = offset(k)
        return lax.rem(z + dz, n_z) * n_x + lax.rem(x + dx, n_x)

    def target(k):
        dz, dx = offset(k)
        return lax.rem(z + n_z - dz, n_z) * n_x + lax.rem(x + n_x - dx, n_x)

    barrier = pltpu.get_barrier_semaphore()

    for k in range(n_ep - 1, 0, -1):
        pl.semaphore_signal(barrier, inc=1, device_id=(target(k), t), device_id_type=MESH)
    near = (sibling, right, left, right2, left2) if ny > 4 else (sibling, right, left)
    for peer in near:
        pl.semaphore_signal(barrier, inc=1, device_id=(ep, peer), device_id_type=MESH)

    loads = [
        (idx_in, idx_v),
        (x_in, xin),
        (mix_in, mixin.at[pl.ds(16, mrows)]),
        (share_in, share_v),
        (gain_in, gain_v),
        (gate_w.at[0], W.at[:, pl.ds(0, hid)]),
        (up_w.at[0], W.at[:, pl.ds(hid, hid)]),
        (down_w.at[0], D),
        (mix_w, MW),
    ]
    loads = [pltpu.make_async_copy(a, b, ld_sem.at[i]) for i, (a, b) in enumerate(loads)]
    for copy in loads:
        copy.start()

    with jax.named_scope("l0"):
        loads[0].wait()
    first, second = idx_v[0:1, :], idx_v[1:2, :]
    experts = lax.broadcasted_iota(jnp.int32, (128, tok), 0)
    named = [(experts == row).astype(F32).astype(BF16) for row in (first, second)]
    before = lax.broadcasted_iota(jnp.int32, (tok, tok), 0) < lax.broadcasted_iota(
        jnp.int32, (tok, tok), 1
    )
    both = named[0] + named[1]
    counts = dot(both, before.astype(F32).astype(BF16)).astype(BF16)
    slot = lax.broadcasted_iota(jnp.int32, (slots, 128), 0)
    owner = lax.broadcasted_iota(jnp.int32, (slots, 128), 1)
    spread = (slot // cap == owner).astype(F32).astype(BF16)
    place = (lax.broadcasted_iota(jnp.int32, (slots, tok), 0) % cap).astype(F32)
    hit = dot(spread, counts) == place
    picks = [
        jnp.where(jnp.logical_and(hit, dot(spread, row) > 0.5), 1.0, 0.0) for row in named
    ]
    with jax.named_scope("l1"):
        loads[1].wait()
    OUT[...] = dot((picks[0] + picks[1]).astype(BF16), xin[...]).astype(BF16)

    with jax.named_scope("l2"):
        loads[2].wait()
    window = lax.shift_left(jnp.int32(2), t // (n_tp // 4))

    def pooled(ext, first_pos):
        total = ext
        for step in (1, 2, 4, 8):
            shifted = pltpu.roll(total, step, 0)
            total = jnp.where(window > step, total + shifted, total)
        rows = ext.shape[0]
        pos = lax.broadcasted_iota(jnp.int32, (rows, ch), 0) + (first_pos - 16)
        div = jnp.minimum(jnp.maximum(pos + 1, 1), window).astype(F32)
        return (total / div - ext)[16:].astype(BF16)

    mixin[0:16, :] = jnp.zeros((16, ch), BF16)
    M[t] = pooled(mixin[...].astype(F32), ep * mrows)
    acc[...] = jnp.zeros(acc.shape, F32)
    sq[...] = jnp.zeros(sq.shape, F32)

    with jax.named_scope("bar"):
        pl.semaphore_wait(barrier, n_ep - 1 + len(near))

    halo_copy = pltpu.make_async_remote_copy(
        src_ref=mixin.at[pl.ds(mrows, 16)],
        dst_ref=halo,
        send_sem=halo_sem.at[0],
        recv_sem=halo_sem.at[1],
        device_id=((ep + 1) % n_ep, t),
        device_id_type=MESH,
    )
    halo_copy.start()

    def ring(rid, buf, rows, nq, skip, ici, d2d):
        cr = rows // nq

        def chunk(block, q):
            return buf.at[block, pl.ds(q * cr, cr)]

        def landed(rel, q):
            return ici.at[rel - 1, q]

        def handed(rel, q):
            return d2d.at[0 if rid == 0 else ny + q if rel == half_ring else rel]

        def push(block, q, peer, recv):
            pltpu.make_async_remote_copy(
                src_ref=chunk(block, q),
                dst_ref=chunk(block, q),
                send_sem=ring_send.at[rid],
                recv_sem=recv,
                device_id=(ep, peer),
                device_id_type=MESH,
            ).start()

        def arrived(ref, recv):
            pltpu.make_async_remote_copy(
                src_ref=ref,
                dst_ref=ref,
                send_sem=ring_send.at[rid],
                recv_sem=recv,
                device_id=(ep, sibling),
                device_id_type=MESH,
            ).wait_recv()

        def begin(q):
            push(t, q, right, landed(1, q))
            push(t, q, left, landed(ny - 1, q))
            push(t, q, sibling, handed(0, q))

        skip = skip if half_ring > 2 else ()
        seen = set()

        def step(s, q):
            if s < half_ring or q % 2 == 0:
                block = 2 * lax.rem(y + ny - s, ny) + core
                arrived(chunk(block, q), landed(s, q))
                if s + 1 < half_ring or (s + 1 == half_ring and q % 2 == 0 and q not in skip):
                    push(block, q, right, landed(s + 1, q))
                if q in skip and s + 2 == half_ring and q % 2 == 0:
                    push(block, q, right2, landed(s + 2, q))
                push(block, q, sibling, handed(s, q))
            if s < half_ring or q % 2 == 1:
                block = 2 * lax.rem(y + s, ny) + core
                arrived(chunk(block, q), landed(ny - s, q))
                if s + 1 < half_ring or (s + 1 == half_ring and q % 2 == 1 and q not in skip):
                    push(block, q, left, landed(ny - s - 1, q))
                if q in skip and s + 2 == half_ring and q % 2 == 1:
                    push(block, q, left2, landed(ny - s - 2, q))
                push(block, q, sibling, handed(ny - s, q))

        def from_sibling(rel, q):
            block = 2 * lax.rem(y + ny - rel, ny) + (1 - core)
            if rel == half_ring:
                arrived(chunk(block, q), handed(rel, q))
            elif rel not in seen:
                seen.add(rel)
                arrived(buf.at[block], handed(rel, q))

        def all_from_sibling():
            arrived(buf.at[pl.ds(0, ny)], handed(0, 0))

        def drain():
            whole = buf.at[pl.ds(0, n_tp - 1)]
            pltpu.make_async_remote_copy(
                src_ref=whole,
                dst_ref=whole,
                send_sem=ring_send.at[rid],
                recv_sem=ici.at[0, 0],
                device_id=(ep, sibling),
                device_id_type=MESH,
            ).wait_send()

        return begin, step, from_sibling, drain, all_from_sibling

    nq = 4
    m_ring = ring(0, M, mrows, 2, (0, 1), m_ici, m_d2d)
    x_ring = ring(1, X, slots, nq, (), ici.at[0], d2d.at[0])
    h_ring = ring(2, H, slots, nq, (2, 3), ici.at[1], d2d.at[1])

    per = n_ep // nq
    for k in range(1, n_ep):
        to = target(k)
        pltpu.make_async_remote_copy(
            src_ref=OUT.at[pl.ds(pl.multiple_of(to * cap, cap), cap)],
            dst_ref=X.at[t, pl.ds(k * cap, cap)],
            send_sem=disp_send,
            recv_sem=disp_recv.at[k // per],
            device_id=(to, t),
            device_id_type=MESH,
        ).start()
    m_ring[0](1)
    X[t, pl.ds(0, cap)] = OUT[pl.ds(pl.multiple_of(ep * cap, cap), cap)]

    def dispatched(q):
        first = max(1, q * per)
        rows = X.at[t, pl.ds(first * cap, ((q + 1) * per - first) * cap)]
        pltpu.make_async_remote_copy(
            src_ref=rows,
            dst_ref=rows,
            send_sem=disp_send,
            recv_sem=disp_recv.at[q],
            device_id=(ep, sibling),
            device_id_type=MESH,
        ).wait_recv()

    loads[3].wait()
    s0, s1 = share_v[0:1, :], share_v[1:2, :]
    total = s0 + s1
    weights = picks[0] * (s0 / total) + picks[1] * (s1 / total)
    high = weights.astype(BF16)
    share_hi[...] = high.astype(F32).T.astype(BF16)
    share_lo[...] = (weights - high.astype(F32)).T.astype(BF16)

    with jax.named_scope("halo"):
        halo_copy.wait_recv()
    past = jnp.where(ep > 0, halo[...].astype(F32), 0.0)
    head = jnp.concatenate([past, mixin[16:32, :].astype(F32)], axis=0)
    M[t, 0:16] = pooled(head, ep * mrows)
    m_ring[0](0)

    for copy in loads[4:]:
        copy.wait()

    tile = slots // nq

    def gather_tile(rel, q):
        x_ring[2](rel, q)
        chip = lax.rem(y + ny - rel, ny)
        cols = pl.ds(pl.multiple_of(chip * 2 * feat, 2 * feat), 2 * feat)
        rows = pl.ds(q * tile, tile)
        value = jnp.concatenate([X[2 * chip, rows], X[2 * chip + 1, rows]], axis=1)
        value = value.astype(F32)
        scaled = (value * gain_v[:, cols]).astype(BF16)
        acc[rows, :] += dot(scaled, W[cols, :])
        square = value * value
        part = square[:, 0:128]
        for j in range(1, 2 * feat // 128):
            part += square[:, j * 128 : (j + 1) * 128]
        sq[rows, :] += part

    def activate(q):
        rows = pl.ds(q * tile, tile)
        inverse = lax.rsqrt(jnp.sum(sq[rows, :], axis=1, keepdims=True) / width + norm_eps)
        gate = acc[rows, 0:hid] * inverse
        up = acc[rows, hid : 2 * hid] * inverse
        H[t, rows] = (gate / (1.0 + jnp.exp(-gate)) * up).astype(BF16)
        acc[rows, :] = jnp.zeros((tile, 2 * hid), F32)

    def down_tile(rel, q):
        h_ring[2](rel, q)
        chip = lax.rem(y + ny - rel, ny)
        cols = pl.ds(pl.multiple_of(chip * 2 * hid, 2 * hid), 2 * hid)
        rows = pl.ds(q * tile, tile)
        value = jnp.concatenate([H[2 * chip, rows], H[2 * chip + 1, rows]], axis=1)
        acc[rows, :] += dot(value, D[cols, :])

    def project(blocks, rows, weight):
        total = None
        for i in range(0, n_tp, 2):
            value = jnp.concatenate([blocks[i, rows], blocks[i + 1, rows]], axis=1)
            depth = value.shape[1]
            term = dot(value, weight[(i // 2) * depth : (i // 2 + 1) * depth, :])
            total = term if total is None else total + term
        return total.astype(BF16)

    def tiles_at(tile_of, distance, q):
        tile_of(distance, q)
        if distance > 0:
            tile_of(ny - distance, q)

    def travel(name, ring, tile_of, first, woven, between, finish):
        for s in range(1, half_ring):
            with jax.named_scope(f"{name}{s}"):
                for q in range(nq):
                    if s == 1:
                        first(q)
                    ring[1](s, q)
                    if woven and s > 1:
                        tiles_at(tile_of, s - 1, q)
                between(s)
                if not woven or s == 1:
                    for q in range(nq):
                        tiles_at(tile_of, s - 1, q)
        with jax.named_scope(f"{name}b"):
            for q in range(nq):
                if woven:
                    tiles_at(tile_of, half_ring - 1, q)
        for group in ((0, 1, 2, 3),) if woven else ((2, 3), (0, 1)):
            with jax.named_scope(f"{name}{half_ring}"):
                for q in group:
                    ring[1](half_ring, q)
            with jax.named_scope(f"{name}end"):
                for q in group:
                    if not woven:
                        tiles_at(tile_of, half_ring - 1, q)
                for q in group:
                    tile_of(half_ring, q)
                    finish(q)

    def begin_hidden(q):
        activate(q)
        h_ring[0](q)

    mixer_steps = [(s, q) for s in range(1, half_ring + 1) for q in (1, 0)]

    def mixer():
        s, q = mixer_steps.pop(0)
        m_ring[1](s, q)

    ahead = 2

    def enter(q):
        if q == 0:
            with jax.named_scope("m11"):
                mixer()
        for p in range(ahead + 1) if q == 0 else range(q + ahead, q + ahead + 1):
            if p < nq:
                with jax.named_scope(f"disp{p}"):
                    dispatched(p)
                x_ring[0](p)

    def give_back(q):
        rows = pl.ds(q * tile, tile)
        Y[rows, :] = acc[rows, :].astype(BF16)
        for k in range(max(1, q * per), (q + 1) * per):
            pltpu.make_async_remote_copy(
                src_ref=Y.at[pl.ds(k * cap, cap)],
                dst_ref=RET.at[pl.ds(pl.multiple_of(ep * cap, cap), cap)],
                send_sem=ret_send,
                recv_sem=ret_recv,
                device_id=(source(k), t),
                device_id_type=MESH,
            ).start()

    def after_rows(s):
        if s == half_ring - 1:
            mixer()

    def after_hidden(s):
        if s == half_ring - 1:
            mixer()
            mixer()

    travel("x", x_ring, gather_tile, enter, True, after_rows, begin_hidden)
    travel("h", h_ring, down_tile, lambda q: None, False, after_hidden, give_back)
    with jax.named_scope("mrest"):
        while mixer_steps:
            mixer()

    m_ring[4]()

    def mix_tile(i, carry):
        rows = pl.ds(pl.multiple_of(i * 128, 128), 128)
        mix_out[rows, :] = project(M, rows, MW)
        return carry

    with jax.named_scope("mixdot"):
        lax.fori_loop(0, mrows // 128, mix_tile, 0)

    RET[pl.ds(pl.multiple_of(ep * cap, cap), cap)] = Y[0:cap]
    back = RET.at[pl.ds(0, slots - cap)]
    with jax.named_scope("retwait"):
        pltpu.make_async_remote_copy(
            src_ref=back,
            dst_ref=back,
            send_sem=ret_send,
            recv_sem=ret_recv,
            device_id=(ep, sibling),
            device_id_type=MESH,
        ).wait_recv()
    with jax.named_scope("combine"):
        exp_out[...] = (dot(share_hi[...], RET[...]) + dot(share_lo[...], RET[...])).astype(BF16)

    with jax.named_scope("drain"):
        halo_copy.wait_send()
        for r in (m_ring, x_ring, h_ring):
            r[3]()
        for buf, sem in ((OUT, disp_send), (Y, ret_send)):
            rows = buf.at[pl.ds(0, slots - cap)]
            pltpu.make_async_remote_copy(
                src_ref=rows,
                dst_ref=rows,
                send_sem=sem,
                recv_sem=ret_recv,
                device_id=(ep, sibling),
                device_id_type=MESH,
            ).wait_send()


def shards(
    n_ep,
    n_tp,
    mix_input,
    mix_weight,
    expert_input,
    expert_index,
    route_share,
    norm_gain,
    gate_weight,
    up_weight,
    down_weight,
):
    mrows, ch = mix_input.shape
    cols = mix_weight.shape[1]
    tok, feat = expert_input.shape
    hid = gate_weight.shape[2]
    out_feat = down_weight.shape[2]
    width = norm_gain.shape[0]
    n_x = 4 if n_ep % 4 == 0 else 1
    slots = 2 * tok * expert_index.shape[1]
    ny = n_tp // 2
    dma = pltpu.SemaphoreType.DMA
    anywhere = pl.BlockSpec(memory_space=pl.ANY)
    return pl.pallas_call(
        functools.partial(kernel, n_ep, n_x, n_tp),
        out_shape=(
            pltpu.VMEM((mrows, cols), BF16),
            pltpu.VMEM((tok, out_feat), BF16),
        ),
        in_specs=[anywhere] * 9,
        out_specs=(pl.BlockSpec(memory_space=pltpu.VMEM),) * 2,
        scratch_shapes=[
            pltpu.VMEM((n_tp, slots, feat), BF16),
            pltpu.VMEM((n_tp, slots, hid), BF16),
            pltpu.VMEM((n_tp, mrows, ch), BF16),
            pltpu.VMEM((width, 2 * hid), BF16),
            pltpu.VMEM((n_tp * hid, out_feat), BF16),
            pltpu.VMEM((n_tp * ch, cols), BF16),
            pltpu.VMEM((tok, feat), BF16),
            pltpu.VMEM((mrows + 16, ch), BF16),
            pltpu.VMEM((16, ch), BF16),
            pltpu.VMEM((2, tok), jnp.int32),
            pltpu.VMEM((2, tok), F32),
            pltpu.VMEM((1, width), F32),
            pltpu.VMEM((slots, feat), BF16),
            pltpu.VMEM((slots, out_feat), BF16),
            pltpu.VMEM((slots, out_feat), BF16),
            pltpu.VMEM((slots, 2 * hid), F32),
            pltpu.VMEM((slots, 128), F32),
            pltpu.VMEM((tok, slots), BF16),
            pltpu.VMEM((tok, slots), BF16),
            dma((9,)),
            dma((3,)),
            dma((2, ny - 1, 4)),
            dma((2, ny + 4)),
            dma((ny - 1, 2)),
            dma((1,)),
            dma,
            dma((4,)),
            dma,
            dma,
            dma((2,)),
        ],
        compiler_params=pltpu.CompilerParams(
            collective_id=0, has_side_effects=True, vmem_limit_bytes=60*2**20
        ),
    )(
        mix_input,
        mix_weight,
        expert_input,
        expert_index.T,
        route_share.T,
        norm_gain.reshape(1, width),
        gate_weight,
        up_weight,
        down_weight,
    )


def solution(mesh):
    placed = (
        P("ep", "tp"),
        P(None, "tp"),
        P("ep", "tp"),
        P("ep", None),
        P("ep", None),
        P(),
        P("ep", None, "tp"),
        P("ep", None, "tp"),
        P("ep", None, "tp"),
    )
    return jax.shard_map(
        functools.partial(shards, mesh.shape["ep"], mesh.shape["tp"]),
        mesh=mesh,
        in_specs=placed,
        out_specs=(P("ep", "tp"), P("ep", "tp")),
        check_vma=False,
    )
```

```python
import functools

import jax
import jax.numpy as jnp
from jax import lax
from jax.experimental import pallas as pl
from jax.experimental.pallas import tpu as pltpu
from jax.sharding import PartitionSpec as P

MESH = pl.DeviceIdType.MESH
F32, BF16 = jnp.float32, jnp.bfloat16
norm_eps = 1e-06


def dot(a, b):
    return jnp.dot(a, b, preferred_element_type=F32)


def kernel(
    n_ep,
    n_x,
    n_tp,
    mix_in,
    mix_w,
    x_in,
    idx_in,
    share_in,
    gain_in,
    gate_w,
    up_w,
    down_w,
    mix_out,
    exp_out,
    X,
    H,
    M,
    W,
    D,
    MW,
    xin,
    mixin,
    halo,
    idx_v,
    share_v,
    gain_v,
    OUT,
    RET,
    Y,
    acc,
    sq,
    share_hi,
    share_lo,
    ld_sem,
    ring_send,
    ici,
    d2d,
    m_ici,
    m_d2d,
    disp_send,
    disp_recv,
    ret_send,
    ret_recv,
    halo_sem,
):
    n_z = n_ep // n_x
    ny = n_tp // 2
    half_ring = ny // 2
    ep, t = lax.axis_index("ep"), lax.axis_index("tp")
    z, x = ep // n_x, ep % n_x
    y, core = t // 2, t % 2
    sibling = 2 * y + (1 - core)
    right = 2 * ((y + 1) % ny) + core
    left = 2 * ((y + ny - 1) % ny) + core
    right2 = 2 * ((y + 2) % ny) + core
    left2 = 2 * ((y + ny - 2) % ny) + core
    cap = OUT.shape[0] // n_ep
    slots = OUT.shape[0]
    half = slots // 2
    tok = xin.shape[0]
    feat = xin.shape[1]
    ch = mixin.shape[1]
    mrows = mix_out.shape[0]
    hid = H.shape[2]
    width = n_tp * feat

    def offset(k):
        i = k // n_x
        return ((i + 1) // 2 if i % 2 else (n_z - i // 2) % n_z), k % n_x

    def source(k):
        dz, dx = offset(k)
        return lax.rem(z + dz, n_z) * n_x + lax.rem(x + dx, n_x)

    def target(k):
        dz, dx = offset(k)
        return lax.rem(z + n_z - dz, n_z) * n_x + lax.rem(x + n_x - dx, n_x)

    loads = [
        (idx_in, idx_v),
        (x_in, xin),
        (mix_in, mixin.at[pl.ds(16, mrows)]),
        (share_in, share_v),
        (gain_in, gain_v),
        (gate_w.at[0], W.at[:, pl.ds(0, hid)]),
        (up_w.at[0], W.at[:, pl.ds(hid, hid)]),
        (down_w.at[0], D),
        (mix_w, MW),
    ]
    loads = [pltpu.make_async_copy(a, b, ld_sem.at[i]) for i, (a, b) in enumerate(loads)]
    for copy in loads[:3]:
        copy.start()

    barrier = pltpu.get_barrier_semaphore()

    for k in range(n_ep - 1, 0, -1):
        pl.semaphore_signal(barrier, inc=1, device_id=(target(k), t), device_id_type=MESH)
    near = (sibling, right, left, right2, left2) if ny > 4 else (sibling, right, left)
    for peer in near:
        pl.semaphore_signal(barrier, inc=1, device_id=(ep, peer), device_id_type=MESH)
    for copy in loads[3:]:
        copy.start()

    with jax.named_scope("l0"):
        loads[0].wait()
    first, second = idx_v[0:1, :], idx_v[1:2, :]
    experts = lax.broadcasted_iota(jnp.int32, (128, tok), 0)
    named = [(experts == row).astype(F32).astype(BF16) for row in (first, second)]
    before = lax.broadcasted_iota(jnp.int32, (tok, tok), 0) < lax.broadcasted_iota(
        jnp.int32, (tok, tok), 1
    )
    both = named[0] + named[1]
    counts = dot(both, before.astype(F32).astype(BF16)).astype(BF16)
    slot = lax.broadcasted_iota(jnp.int32, (slots, 128), 0)
    owner = lax.broadcasted_iota(jnp.int32, (slots, 128), 1)
    spread = (slot // cap == owner).astype(F32).astype(BF16)
    place = (lax.broadcasted_iota(jnp.int32, (slots, tok), 0) % cap).astype(F32)
    hit = dot(spread, counts) == place
    picks = [
        jnp.where(jnp.logical_and(hit, dot(spread, row) > 0.5), 1.0, 0.0) for row in named
    ]
    with jax.named_scope("l1"):
        loads[1].wait()
    OUT[...] = dot((picks[0] + picks[1]).astype(BF16), xin[...]).astype(BF16)

    with jax.named_scope("l2"):
        loads[2].wait()
    window = lax.shift_left(jnp.int32(2), t // (n_tp // 4))

    def pooled(ext, first_pos):
        total = ext
        for step in (1, 2, 4, 8):
            shifted = pltpu.roll(total, step, 0)
            total = jnp.where(window > step, total + shifted, total)
        rows = ext.shape[0]
        pos = lax.broadcasted_iota(jnp.int32, (rows, ch), 0) + (first_pos - 16)
        div = jnp.minimum(jnp.maximum(pos + 1, 1), window).astype(F32)
        return (total / div - ext)[16:].astype(BF16)

    mixin[0:16, :] = jnp.zeros((16, ch), BF16)
    M[t] = pooled(mixin[...].astype(F32), ep * mrows)
    acc[...] = jnp.zeros(acc.shape, F32)
    sq[...] = jnp.zeros(sq.shape, F32)

    with jax.named_scope("bar"):
        pl.semaphore_wait(barrier, n_ep - 1 + len(near))

    halo_copy = pltpu.make_async_remote_copy(
        src_ref=mixin.at[pl.ds(mrows, 16)],
        dst_ref=halo,
        send_sem=halo_sem.at[0],
        recv_sem=halo_sem.at[1],
        device_id=((ep + 1) % n_ep, t),
        device_id_type=MESH,
    )
    halo_copy.start()

    def ring(rid, buf, rows, nq, skip, ici, d2d):
        cr = rows // nq

        def chunk(block, q):
            return buf.at[block, pl.ds(q * cr, cr)]

        def landed(rel, q):
            return ici.at[rel - 1, q]

        def handed(rel, q):
            return d2d.at[0 if rid == 0 else ny + q if rel == half_ring else rel]

        def push(block, q, peer, recv):
            pltpu.make_async_remote_copy(
                src_ref=chunk(block, q),
                dst_ref=chunk(block, q),
                send_sem=ring_send.at[rid],
                recv_sem=recv,
                device_id=(ep, peer),
                device_id_type=MESH,
            ).start()

        def arrived(ref, recv):
            pltpu.make_async_remote_copy(
                src_ref=ref,
                dst_ref=ref,
                send_sem=ring_send.at[rid],
                recv_sem=recv,
                device_id=(ep, sibling),
                device_id_type=MESH,
            ).wait_recv()

        def begin(q):
            push(t, q, right, landed(1, q))
            push(t, q, left, landed(ny - 1, q))
            push(t, q, sibling, handed(0, q))

        skip = skip if half_ring > 2 else ()
        seen = set()

        def step(s, q):
            if s < half_ring or q % 2 == 0:
                block = 2 * lax.rem(y + ny - s, ny) + core
                arrived(chunk(block, q), landed(s, q))
                if s + 1 < half_ring or (s + 1 == half_ring and q % 2 == 0 and q not in skip):
                    push(block, q, right, landed(s + 1, q))
                if q in skip and s + 2 == half_ring and q % 2 == 0:
                    push(block, q, right2, landed(s + 2, q))
                push(block, q, sibling, handed(s, q))
            if s < half_ring or q % 2 == 1:
                block = 2 * lax.rem(y + s, ny) + core
                arrived(chunk(block, q), landed(ny - s, q))
                if s + 1 < half_ring or (s + 1 == half_ring and q % 2 == 1 and q not in skip):
                    push(block, q, left, landed(ny - s - 1, q))
                if q in skip and s + 2 == half_ring and q % 2 == 1:
                    push(block, q, left2, landed(ny - s - 2, q))
                push(block, q, sibling, handed(ny - s, q))

        def from_sibling(rel, q):
            block = 2 * lax.rem(y + ny - rel, ny) + (1 - core)
            if rel == half_ring:
                arrived(chunk(block, q), handed(rel, q))
            elif rel not in seen:
                seen.add(rel)
                arrived(buf.at[block], handed(rel, q))

        def all_from_sibling():
            arrived(buf.at[pl.ds(0, ny)], handed(0, 0))

        def drain():
            whole = buf.at[pl.ds(0, n_tp - 1)]
            pltpu.make_async_remote_copy(
                src_ref=whole,
                dst_ref=whole,
                send_sem=ring_send.at[rid],
                recv_sem=ici.at[0, 0],
                device_id=(ep, sibling),
                device_id_type=MESH,
            ).wait_send()

        return begin, step, from_sibling, drain, all_from_sibling

    nq = 4
    m_ring = ring(0, M, mrows, 2, (0, 1), m_ici, m_d2d)
    x_ring = ring(1, X, slots, nq, (), ici.at[0], d2d.at[0])
    h_ring = ring(2, H, slots, nq, (2, 3), ici.at[1], d2d.at[1])

    per = n_ep // nq
    for k in range(1, n_ep):
        to = target(k)
        pltpu.make_async_remote_copy(
            src_ref=OUT.at[pl.ds(pl.multiple_of(to * cap, cap), cap)],
            dst_ref=X.at[t, pl.ds(k * cap, cap)],
            send_sem=disp_send,
            recv_sem=disp_recv.at[k // per],
            device_id=(to, t),
            device_id_type=MESH,
        ).start()
    m_ring[0](1)
    X[t, pl.ds(0, cap)] = OUT[pl.ds(pl.multiple_of(ep * cap, cap), cap)]

    def dispatched(q):
        first = max(1, q * per)
        rows = X.at[t, pl.ds(first * cap, ((q + 1) * per - first) * cap)]
        pltpu.make_async_remote_copy(
            src_ref=rows,
            dst_ref=rows,
            send_sem=disp_send,
            recv_sem=disp_recv.at[q],
            device_id=(ep, sibling),
            device_id_type=MESH,
        ).wait_recv()

    loads[3].wait()
    s0, s1 = share_v[0:1, :], share_v[1:2, :]
    total = s0 + s1
    weights = picks[0] * (s0 / total) + picks[1] * (s1 / total)
    high = weights.astype(BF16)
    share_hi[...] = high.astype(F32).T.astype(BF16)
    share_lo[...] = (weights - high.astype(F32)).T.astype(BF16)

    with jax.named_scope("halo"):
        halo_copy.wait_recv()
    past = jnp.where(ep > 0, halo[...].astype(F32), 0.0)
    head = jnp.concatenate([past, mixin[16:32, :].astype(F32)], axis=0)
    M[t, 0:16] = pooled(head, ep * mrows)
    m_ring[0](0)

    for copy in loads[4:]:
        copy.wait()

    tile = slots // nq

    def gather_tile(rel, q):
        x_ring[2](rel, q)
        chip = lax.rem(y + ny - rel, ny)
        cols = pl.ds(pl.multiple_of(chip * 2 * feat, 2 * feat), 2 * feat)
        rows = pl.ds(q * tile, tile)
        value = jnp.concatenate([X[2 * chip, rows], X[2 * chip + 1, rows]], axis=1)
        value = value.astype(F32)
        scaled = (value * gain_v[:, cols]).astype(BF16)
        acc[rows, :] += dot(scaled, W[cols, :])
        square = value * value
        part = square[:, 0:128]
        for j in range(1, 2 * feat // 128):
            part += square[:, j * 128 : (j + 1) * 128]
        sq[rows, :] += part

    def activate(q):
        rows = pl.ds(q * tile, tile)
        inverse = lax.rsqrt(jnp.sum(sq[rows, :], axis=1, keepdims=True) / width + norm_eps)
        gate = acc[rows, 0:hid] * inverse
        up = acc[rows, hid : 2 * hid] * inverse
        H[t, rows] = (gate / (1.0 + jnp.exp(-gate)) * up).astype(BF16)
        acc[rows, :] = jnp.zeros((tile, 2 * hid), F32)

    def down_tile(rel, q):
        h_ring[2](rel, q)
        chip = lax.rem(y + ny - rel, ny)
        cols = pl.ds(pl.multiple_of(chip * 2 * hid, 2 * hid), 2 * hid)
        rows = pl.ds(q * tile, tile)
        value = jnp.concatenate([H[2 * chip, rows], H[2 * chip + 1, rows]], axis=1)
        acc[rows, :] += dot(value, D[cols, :])

    def project(blocks, rows, weight):
        total = None
        for i in range(0, n_tp, 2):
            value = jnp.concatenate([blocks[i, rows], blocks[i + 1, rows]], axis=1)
            depth = value.shape[1]
            term = dot(value, weight[(i // 2) * depth : (i // 2 + 1) * depth, :])
            total = term if total is None else total + term
        return total.astype(BF16)

    def tiles_at(tile_of, distance, q):
        tile_of(distance, q)
        if distance > 0:
            tile_of(ny - distance, q)

    def travel(name, ring, tile_of, first, woven, between, finish):
        for s in range(1, half_ring):
            with jax.named_scope(f"{name}{s}"):
                for q in range(nq):
                    if s == 1:
                        first(q)
                    ring[1](s, q)
                    if woven and s > 1:
                        tiles_at(tile_of, s - 1, q)
                between(s)
                if not woven or s == 1:
                    for q in range(nq):
                        tiles_at(tile_of, s - 1, q)
        with jax.named_scope(f"{name}b"):
            for q in range(nq):
                if woven:
                    tiles_at(tile_of, half_ring - 1, q)
        for group in ((0, 1, 2, 3),) if woven else ((2, 3), (0, 1)):
            with jax.named_scope(f"{name}{half_ring}"):
                for q in group:
                    ring[1](half_ring, q)
            with jax.named_scope(f"{name}end"):
                for q in group:
                    if not woven:
                        tiles_at(tile_of, half_ring - 1, q)
                for q in group:
                    tile_of(half_ring, q)
                    finish(q)

    def begin_hidden(q):
        activate(q)
        h_ring[0](q)

    mixer_steps = [(s, q) for s in range(1, half_ring + 1) for q in (1, 0)]

    def mixer():
        s, q = mixer_steps.pop(0)
        m_ring[1](s, q)

    ahead = 2

    def enter(q):
        for p in range(ahead + 1) if q == 0 else range(q + ahead, q + ahead + 1):
            if p < nq:
                with jax.named_scope(f"disp{p}"):
                    dispatched(p)
                x_ring[0](p)
            if p == 0:
                with jax.named_scope("m11"):
                    mixer()

    def give_back(q):
        rows = pl.ds(q * tile, tile)
        Y[rows, :] = acc[rows, :].astype(BF16)
        for k in range(max(1, q * per), (q + 1) * per):
            pltpu.make_async_remote_copy(
                src_ref=Y.at[pl.ds(k * cap, cap)],
                dst_ref=RET.at[pl.ds(pl.multiple_of(ep * cap, cap), cap)],
                send_sem=ret_send,
                recv_sem=ret_recv,
                device_id=(source(k), t),
                device_id_type=MESH,
            ).start()

    def after_rows(s):
        if s == half_ring - 1:
            mixer()

    def after_hidden(s):
        if s == half_ring - 1:
            mixer()
            mixer()

    travel("x", x_ring, gather_tile, enter, True, after_rows, begin_hidden)
    travel("h", h_ring, down_tile, lambda q: None, False, after_hidden, give_back)
    with jax.named_scope("mrest"):
        while mixer_steps:
            mixer()

    m_ring[4]()

    def mix_tile(i, carry):
        rows = pl.ds(pl.multiple_of(i * 128, 128), 128)
        mix_out[rows, :] = project(M, rows, MW)
        return carry

    with jax.named_scope("mixdot"):
        lax.fori_loop(0, mrows // 128, mix_tile, 0)

    RET[pl.ds(pl.multiple_of(ep * cap, cap), cap)] = Y[0:cap]
    back = RET.at[pl.ds(0, slots - cap)]
    with jax.named_scope("retwait"):
        pltpu.make_async_remote_copy(
            src_ref=back,
            dst_ref=back,
            send_sem=ret_send,
            recv_sem=ret_recv,
            device_id=(ep, sibling),
            device_id_type=MESH,
        ).wait_recv()
    with jax.named_scope("combine"):
        exp_out[...] = (dot(share_hi[...], RET[...]) + dot(share_lo[...], RET[...])).astype(BF16)

    with jax.named_scope("drain"):
        halo_copy.wait_send()
        for r in (m_ring, x_ring, h_ring):
            r[3]()
        for buf, sem in ((OUT, disp_send), (Y, ret_send)):
            rows = buf.at[pl.ds(0, slots - cap)]
            pltpu.make_async_remote_copy(
                src_ref=rows,
                dst_ref=rows,
                send_sem=sem,
                recv_sem=ret_recv,
                device_id=(ep, sibling),
                device_id_type=MESH,
            ).wait_send()


def shards(
    n_ep,
    n_tp,
    mix_input,
    mix_weight,
    expert_input,
    expert_index,
    route_share,
    norm_gain,
    gate_weight,
    up_weight,
    down_weight,
):
    mrows, ch = mix_input.shape
    cols = mix_weight.shape[1]
    tok, feat = expert_input.shape
    hid = gate_weight.shape[2]
    out_feat = down_weight.shape[2]
    width = norm_gain.shape[0]
    n_x = 4 if n_ep % 4 == 0 else 1
    slots = 2 * tok * expert_index.shape[1]
    ny = n_tp // 2
    dma = pltpu.SemaphoreType.DMA
    anywhere = pl.BlockSpec(memory_space=pl.ANY)
    return pl.pallas_call(
        functools.partial(kernel, n_ep, n_x, n_tp),
        out_shape=(
            pltpu.VMEM((mrows, cols), BF16),
            pltpu.VMEM((tok, out_feat), BF16),
        ),
        in_specs=[anywhere] * 9,
        out_specs=(pl.BlockSpec(memory_space=pltpu.VMEM),) * 2,
        scratch_shapes=[
            pltpu.VMEM((n_tp, slots, feat), BF16),
            pltpu.VMEM((n_tp, slots, hid), BF16),
            pltpu.VMEM((n_tp, mrows, ch), BF16),
            pltpu.VMEM((width, 2 * hid), BF16),
            pltpu.VMEM((n_tp * hid, out_feat), BF16),
            pltpu.VMEM((n_tp * ch, cols), BF16),
            pltpu.VMEM((tok, feat), BF16),
            pltpu.VMEM((mrows + 16, ch), BF16),
            pltpu.VMEM((16, ch), BF16),
            pltpu.VMEM((2, tok), jnp.int32),
            pltpu.VMEM((2, tok), F32),
            pltpu.VMEM((1, width), F32),
            pltpu.VMEM((slots, feat), BF16),
            pltpu.VMEM((slots, out_feat), BF16),
            pltpu.VMEM((slots, out_feat), BF16),
            pltpu.VMEM((slots, 2 * hid), F32),
            pltpu.VMEM((slots, 128), F32),
            pltpu.VMEM((tok, slots), BF16),
            pltpu.VMEM((tok, slots), BF16),
            dma((9,)),
            dma((3,)),
            dma((2, ny - 1, 4)),
            dma((2, ny + 4)),
            dma((ny - 1, 2)),
            dma((1,)),
            dma,
            dma((4,)),
            dma,
            dma,
            dma((2,)),
        ],
        compiler_params=pltpu.CompilerParams(
            collective_id=0, has_side_effects=True, vmem_limit_bytes=60*2**20
        ),
    )(
        mix_input,
        mix_weight,
        expert_input,
        expert_index.T,
        route_share.T,
        norm_gain.reshape(1, width),
        gate_weight,
        up_weight,
        down_weight,
    )


def solution(mesh):
    placed = (
        P("ep", "tp"),
        P(None, "tp"),
        P("ep", "tp"),
        P("ep", None),
        P("ep", None),
        P(),
        P("ep", None, "tp"),
        P("ep", None, "tp"),
        P("ep", None, "tp"),
    )
    return jax.shard_map(
        functools.partial(shards, mesh.shape["ep"], mesh.shape["tp"]),
        mesh=mesh,
        in_specs=placed,
        out_specs=(P("ep", "tp"), P("ep", "tp")),
        check_vma=False,
    )
```

```python
import functools

import jax
import jax.numpy as jnp
from jax import lax
from jax.experimental import pallas as pl
from jax.experimental.pallas import tpu as pltpu
from jax.sharding import PartitionSpec as P

MESH = pl.DeviceIdType.MESH
F32, BF16 = jnp.float32, jnp.bfloat16
norm_eps = 1e-06


def dot(a, b):
    return jnp.dot(a, b, preferred_element_type=F32)


def kernel(
    n_ep,
    n_x,
    n_tp,
    mix_in,
    mix_w,
    x_in,
    idx_in,
    share_in,
    gain_in,
    gate_w,
    up_w,
    down_w,
    mix_out,
    exp_out,
    X,
    H,
    M,
    W,
    D,
    MW,
    xin,
    mixin,
    halo,
    idx_v,
    share_v,
    gain_v,
    OUT,
    RET,
    Y,
    acc,
    sq,
    share_hi,
    share_lo,
    ld_sem,
    ring_send,
    ici,
    d2d,
    m_ici,
    m_d2d,
    disp_send,
    disp_recv,
    ret_send,
    ret_recv,
    halo_sem,
):
    n_z = n_ep // n_x
    ny = n_tp // 2
    half_ring = ny // 2
    ep, t = lax.axis_index("ep"), lax.axis_index("tp")
    z, x = ep // n_x, ep % n_x
    y, core = t // 2, t % 2
    sibling = 2 * y + (1 - core)
    right = 2 * ((y + 1) % ny) + core
    left = 2 * ((y + ny - 1) % ny) + core
    right2 = 2 * ((y + 2) % ny) + core
    left2 = 2 * ((y + ny - 2) % ny) + core
    cap = OUT.shape[0] // n_ep
    slots = OUT.shape[0]
    half = slots // 2
    tok = xin.shape[0]
    feat = xin.shape[1]
    ch = mixin.shape[1]
    mrows = mix_out.shape[0]
    hid = H.shape[2]
    width = n_tp * feat

    def offset(k):
        i = k // n_x
        return ((i + 1) // 2 if i % 2 else (n_z - i // 2) % n_z), k % n_x

    def source(k):
        dz, dx = offset(k)
        return lax.rem(z + dz, n_z) * n_x + lax.rem(x + dx, n_x)

    def target(k):
        dz, dx = offset(k)
        return lax.rem(z + n_z - dz, n_z) * n_x + lax.rem(x + n_x - dx, n_x)

    loads = [
        (idx_in, idx_v),
        (x_in, xin),
        (mix_in, mixin.at[pl.ds(16, mrows)]),
        (share_in, share_v),
        (gain_in, gain_v),
        (gate_w.at[0], W.at[:, pl.ds(0, hid)]),
        (up_w.at[0], W.at[:, pl.ds(hid, hid)]),
        (down_w.at[0], D),
        (mix_w, MW),
    ]
    loads = [pltpu.make_async_copy(a, b, ld_sem.at[i]) for i, (a, b) in enumerate(loads)]
    for copy in loads[:3]:
        copy.start()

    barrier = pltpu.get_barrier_semaphore()

    for k in range(n_ep - 1, 0, -1):
        pl.semaphore_signal(barrier, inc=1, device_id=(target(k), t), device_id_type=MESH)
    near = (sibling, right, left, right2, left2) if ny > 4 else (sibling, right, left)
    for peer in near:
        pl.semaphore_signal(barrier, inc=1, device_id=(ep, peer), device_id_type=MESH)
    for copy in loads[3:]:
        copy.start()

    with jax.named_scope("l0"):
        loads[0].wait()
    first, second = idx_v[0:1, :], idx_v[1:2, :]
    experts = lax.broadcasted_iota(jnp.int32, (128, tok), 0)
    named = [(experts == row).astype(F32).astype(BF16) for row in (first, second)]
    before = lax.broadcasted_iota(jnp.int32, (tok, tok), 0) < lax.broadcasted_iota(
        jnp.int32, (tok, tok), 1
    )
    both = named[0] + named[1]
    counts = dot(both, before.astype(F32).astype(BF16)).astype(BF16)
    slot = lax.broadcasted_iota(jnp.int32, (slots, 128), 0)
    owner = lax.broadcasted_iota(jnp.int32, (slots, 128), 1)
    spread = (slot // cap == owner).astype(F32).astype(BF16)
    place = (lax.broadcasted_iota(jnp.int32, (slots, tok), 0) % cap).astype(F32)
    hit = dot(spread, counts) == place
    picks = [
        jnp.where(jnp.logical_and(hit, dot(spread, row) > 0.5), 1.0, 0.0) for row in named
    ]
    with jax.named_scope("l1"):
        loads[1].wait()
    OUT[...] = dot((picks[0] + picks[1]).astype(BF16), xin[...]).astype(BF16)

    with jax.named_scope("l2"):
        loads[2].wait()
    window = lax.shift_left(jnp.int32(2), t // (n_tp // 4))

    def pooled(ext, first_pos):
        total = ext
        for step in (1, 2, 4, 8):
            shifted = pltpu.roll(total, step, 0)
            total = jnp.where(window > step, total + shifted, total)
        rows = ext.shape[0]
        pos = lax.broadcasted_iota(jnp.int32, (rows, ch), 0) + (first_pos - 16)
        div = jnp.minimum(jnp.maximum(pos + 1, 1), window).astype(F32)
        return (total / div - ext)[16:].astype(BF16)

    mixin[0:16, :] = jnp.zeros((16, ch), BF16)
    M[t] = pooled(mixin[...].astype(F32), ep * mrows)
    acc[...] = jnp.zeros(acc.shape, F32)
    sq[...] = jnp.zeros(sq.shape, F32)

    with jax.named_scope("bar"):
        pl.semaphore_wait(barrier, n_ep - 1 + len(near))

    halo_copy = pltpu.make_async_remote_copy(
        src_ref=mixin.at[pl.ds(mrows, 16)],
        dst_ref=halo,
        send_sem=halo_sem.at[0],
        recv_sem=halo_sem.at[1],
        device_id=((ep + 1) % n_ep, t),
        device_id_type=MESH,
    )
    halo_copy.start()

    def ring(rid, buf, rows, nq, skip, ici, d2d):
        cr = rows // nq

        def chunk(block, q):
            return buf.at[block, pl.ds(q * cr, cr)]

        def landed(rel, q):
            return ici.at[rel - 1, q]

        def handed(rel, q):
            return d2d.at[0 if rid == 0 else ny + q if rel == half_ring else rel]

        def push(block, q, peer, recv):
            pltpu.make_async_remote_copy(
                src_ref=chunk(block, q),
                dst_ref=chunk(block, q),
                send_sem=ring_send.at[rid],
                recv_sem=recv,
                device_id=(ep, peer),
                device_id_type=MESH,
            ).start()

        def arrived(ref, recv):
            pltpu.make_async_remote_copy(
                src_ref=ref,
                dst_ref=ref,
                send_sem=ring_send.at[rid],
                recv_sem=recv,
                device_id=(ep, sibling),
                device_id_type=MESH,
            ).wait_recv()

        def begin(q):
            push(t, q, right, landed(1, q))
            push(t, q, left, landed(ny - 1, q))
            push(t, q, sibling, handed(0, q))

        skip = skip if half_ring > 2 else ()
        seen = set()

        def step(s, q):
            if s < half_ring or q % 2 == 0:
                block = 2 * lax.rem(y + ny - s, ny) + core
                arrived(chunk(block, q), landed(s, q))
                if s + 1 < half_ring or (s + 1 == half_ring and q % 2 == 0 and q not in skip):
                    push(block, q, right, landed(s + 1, q))
                if q in skip and s + 2 == half_ring and q % 2 == 0:
                    push(block, q, right2, landed(s + 2, q))
                push(block, q, sibling, handed(s, q))
            if s < half_ring or q % 2 == 1:
                block = 2 * lax.rem(y + s, ny) + core
                arrived(chunk(block, q), landed(ny - s, q))
                if s + 1 < half_ring or (s + 1 == half_ring and q % 2 == 1 and q not in skip):
                    push(block, q, left, landed(ny - s - 1, q))
                if q in skip and s + 2 == half_ring and q % 2 == 1:
                    push(block, q, left2, landed(ny - s - 2, q))
                push(block, q, sibling, handed(ny - s, q))

        def from_sibling(rel, q):
            block = 2 * lax.rem(y + ny - rel, ny) + (1 - core)
            if rel == half_ring:
                arrived(chunk(block, q), handed(rel, q))
            elif rel not in seen:
                seen.add(rel)
                arrived(buf.at[block], handed(rel, q))

        def all_from_sibling():
            arrived(buf.at[pl.ds(0, ny)], handed(0, 0))

        def drain():
            whole = buf.at[pl.ds(0, n_tp - 1)]
            pltpu.make_async_remote_copy(
                src_ref=whole,
                dst_ref=whole,
                send_sem=ring_send.at[rid],
                recv_sem=ici.at[0, 0],
                device_id=(ep, sibling),
                device_id_type=MESH,
            ).wait_send()

        return begin, step, from_sibling, drain, all_from_sibling

    nq = 4
    m_ring = ring(0, M, mrows, 2, (0, 1), m_ici, m_d2d)
    x_ring = ring(1, X, slots, nq, (), ici.at[0], d2d.at[0])
    h_ring = ring(2, H, slots, nq, (2, 3), ici.at[1], d2d.at[1])

    per = n_ep // nq
    for k in range(1, n_ep):
        to = target(k)
        pltpu.make_async_remote_copy(
            src_ref=OUT.at[pl.ds(pl.multiple_of(to * cap, cap), cap)],
            dst_ref=X.at[t, pl.ds(k * cap, cap)],
            send_sem=disp_send,
            recv_sem=disp_recv.at[k // per],
            device_id=(to, t),
            device_id_type=MESH,
        ).start()
    m_ring[0](1)
    X[t, pl.ds(0, cap)] = OUT[pl.ds(pl.multiple_of(ep * cap, cap), cap)]

    def dispatched(q):
        first = max(1, q * per)
        rows = X.at[t, pl.ds(first * cap, ((q + 1) * per - first) * cap)]
        pltpu.make_async_remote_copy(
            src_ref=rows,
            dst_ref=rows,
            send_sem=disp_send,
            recv_sem=disp_recv.at[q],
            device_id=(ep, sibling),
            device_id_type=MESH,
        ).wait_recv()

    loads[3].wait()
    s0, s1 = share_v[0:1, :], share_v[1:2, :]
    total = s0 + s1
    weights = picks[0] * (s0 / total) + picks[1] * (s1 / total)
    high = weights.astype(BF16)
    share_hi[...] = high.astype(F32).T.astype(BF16)
    share_lo[...] = (weights - high.astype(F32)).T.astype(BF16)

    with jax.named_scope("halo"):
        halo_copy.wait_recv()
    past = jnp.where(ep > 0, halo[...].astype(F32), 0.0)
    head = jnp.concatenate([past, mixin[16:32, :].astype(F32)], axis=0)
    M[t, 0:16] = pooled(head, ep * mrows)
    m_ring[0](0)

    for copy in loads[4:]:
        copy.wait()

    tile = slots // nq

    def gather_tile(rel, q):
        x_ring[2](rel, q)
        chip = lax.rem(y + ny - rel, ny)
        cols = pl.ds(pl.multiple_of(chip * 2 * feat, 2 * feat), 2 * feat)
        rows = pl.ds(q * tile, tile)
        value = jnp.concatenate([X[2 * chip, rows], X[2 * chip + 1, rows]], axis=1)
        value = value.astype(F32)
        scaled = (value * gain_v[:, cols]).astype(BF16)
        acc[rows, :] += dot(scaled, W[cols, :])
        square = value * value
        part = square[:, 0:128]
        for j in range(1, 2 * feat // 128):
            part += square[:, j * 128 : (j + 1) * 128]
        sq[rows, :] += part

    def activate(q):
        rows = pl.ds(q * tile, tile)
        inverse = lax.rsqrt(jnp.sum(sq[rows, :], axis=1, keepdims=True) / width + norm_eps)
        gate = acc[rows, 0:hid] * inverse
        up = acc[rows, hid : 2 * hid] * inverse
        H[t, rows] = (gate / (1.0 + jnp.exp(-gate)) * up).astype(BF16)
        acc[rows, :] = jnp.zeros((tile, 2 * hid), F32)

    def down_tile(rel, q):
        h_ring[2](rel, q)
        chip = lax.rem(y + ny - rel, ny)
        cols = pl.ds(pl.multiple_of(chip * 2 * hid, 2 * hid), 2 * hid)
        rows = pl.ds(q * tile, tile)
        value = jnp.concatenate([H[2 * chip, rows], H[2 * chip + 1, rows]], axis=1)
        acc[rows, :] += dot(value, D[cols, :])

    def project(blocks, rows, weight):
        total = None
        for i in range(0, n_tp, 2):
            value = jnp.concatenate([blocks[i, rows], blocks[i + 1, rows]], axis=1)
            depth = value.shape[1]
            term = dot(value, weight[(i // 2) * depth : (i // 2 + 1) * depth, :])
            total = term if total is None else total + term
        return total.astype(BF16)

    def tiles_at(tile_of, distance, q):
        tile_of(distance, q)
        if distance > 0:
            tile_of(ny - distance, q)

    def travel(name, ring, tile_of, first, woven, between, finish):
        for s in range(1, half_ring):
            with jax.named_scope(f"{name}{s}"):
                for q in range(nq):
                    if s == 1:
                        first(q)
                    ring[1](s, q)
                    if woven and s > 1:
                        tiles_at(tile_of, s - 1, q)
                between(s)
                if not woven or s == 1:
                    for q in range(nq):
                        tiles_at(tile_of, s - 1, q)
        with jax.named_scope(f"{name}b"):
            for q in range(nq):
                if woven:
                    tiles_at(tile_of, half_ring - 1, q)
        for group in ((0, 1, 2, 3),) if woven else ((3, 2), (1, 0)):
            with jax.named_scope(f"{name}{half_ring}"):
                for q in group:
                    ring[1](half_ring, q)
            with jax.named_scope(f"{name}end"):
                for q in group:
                    if not woven:
                        tiles_at(tile_of, half_ring - 1, q)
                for q in group:
                    tile_of(half_ring, q)
                    finish(q)

    def begin_hidden(q):
        activate(q)
        h_ring[0](q)

    mixer_steps = [(s, q) for s in range(1, half_ring + 1) for q in (1, 0)]

    def mixer():
        s, q = mixer_steps.pop(0)
        m_ring[1](s, q)

    ahead = 2

    def enter(q):
        for p in range(ahead + 1) if q == 0 else range(q + ahead, q + ahead + 1):
            if p < nq:
                with jax.named_scope(f"disp{p}"):
                    dispatched(p)
                x_ring[0](p)
            if p == 0:
                with jax.named_scope("m11"):
                    mixer()

    def give_back(q):
        rows = pl.ds(q * tile, tile)
        Y[rows, :] = acc[rows, :].astype(BF16)
        for k in reversed(range(max(1, q * per), (q + 1) * per)):
            pltpu.make_async_remote_copy(
                src_ref=Y.at[pl.ds(k * cap, cap)],
                dst_ref=RET.at[pl.ds(pl.multiple_of(ep * cap, cap), cap)],
                send_sem=ret_send,
                recv_sem=ret_recv,
                device_id=(source(k), t),
                device_id_type=MESH,
            ).start()

    def after_rows(s):
        if s == half_ring - 1:
            mixer()

    def after_hidden(s):
        if s == half_ring - 1:
            mixer()
            mixer()

    travel("x", x_ring, gather_tile, enter, True, after_rows, begin_hidden)
    travel("h", h_ring, down_tile, lambda q: None, False, after_hidden, give_back)
    with jax.named_scope("mrest"):
        while mixer_steps:
            mixer()

    m_ring[4]()

    def mix_tile(i, carry):
        rows = pl.ds(pl.multiple_of(i * 128, 128), 128)
        mix_out[rows, :] = project(M, rows, MW)
        return carry

    with jax.named_scope("mixdot"):
        lax.fori_loop(0, mrows // 128, mix_tile, 0)

    RET[pl.ds(pl.multiple_of(ep * cap, cap), cap)] = Y[0:cap]
    back = RET.at[pl.ds(0, slots - cap)]
    with jax.named_scope("retwait"):
        pltpu.make_async_remote_copy(
            src_ref=back,
            dst_ref=back,
            send_sem=ret_send,
            recv_sem=ret_recv,
            device_id=(ep, sibling),
            device_id_type=MESH,
        ).wait_recv()
    with jax.named_scope("combine"):
        exp_out[...] = (dot(share_hi[...], RET[...]) + dot(share_lo[...], RET[...])).astype(BF16)

    with jax.named_scope("drain"):
        halo_copy.wait_send()
        for r in (m_ring, x_ring, h_ring):
            r[3]()
        for buf, sem in ((OUT, disp_send), (Y, ret_send)):
            rows = buf.at[pl.ds(0, slots - cap)]
            pltpu.make_async_remote_copy(
                src_ref=rows,
                dst_ref=rows,
                send_sem=sem,
                recv_sem=ret_recv,
                device_id=(ep, sibling),
                device_id_type=MESH,
            ).wait_send()


def shards(
    n_ep,
    n_tp,
    mix_input,
    mix_weight,
    expert_input,
    expert_index,
    route_share,
    norm_gain,
    gate_weight,
    up_weight,
    down_weight,
):
    mrows, ch = mix_input.shape
    cols = mix_weight.shape[1]
    tok, feat = expert_input.shape
    hid = gate_weight.shape[2]
    out_feat = down_weight.shape[2]
    width = norm_gain.shape[0]
    n_x = 4 if n_ep % 4 == 0 else 1
    slots = 2 * tok * expert_index.shape[1]
    ny = n_tp // 2
    dma = pltpu.SemaphoreType.DMA
    anywhere = pl.BlockSpec(memory_space=pl.ANY)
    return pl.pallas_call(
        functools.partial(kernel, n_ep, n_x, n_tp),
        out_shape=(
            pltpu.VMEM((mrows, cols), BF16),
            pltpu.VMEM((tok, out_feat), BF16),
        ),
        in_specs=[anywhere] * 9,
        out_specs=(pl.BlockSpec(memory_space=pltpu.VMEM),) * 2,
        scratch_shapes=[
            pltpu.VMEM((n_tp, slots, feat), BF16),
            pltpu.VMEM((n_tp, slots, hid), BF16),
            pltpu.VMEM((n_tp, mrows, ch), BF16),
            pltpu.VMEM((width, 2 * hid), BF16),
            pltpu.VMEM((n_tp * hid, out_feat), BF16),
            pltpu.VMEM((n_tp * ch, cols), BF16),
            pltpu.VMEM((tok, feat), BF16),
            pltpu.VMEM((mrows + 16, ch), BF16),
            pltpu.VMEM((16, ch), BF16),
            pltpu.VMEM((2, tok), jnp.int32),
            pltpu.VMEM((2, tok), F32),
            pltpu.VMEM((1, width), F32),
            pltpu.VMEM((slots, feat), BF16),
            pltpu.VMEM((slots, out_feat), BF16),
            pltpu.VMEM((slots, out_feat), BF16),
            pltpu.VMEM((slots, 2 * hid), F32),
            pltpu.VMEM((slots, 128), F32),
            pltpu.VMEM((tok, slots), BF16),
            pltpu.VMEM((tok, slots), BF16),
            dma((9,)),
            dma((3,)),
            dma((2, ny - 1, 4)),
            dma((2, ny + 4)),
            dma((ny - 1, 2)),
            dma((1,)),
            dma,
            dma((4,)),
            dma,
            dma,
            dma((2,)),
        ],
        compiler_params=pltpu.CompilerParams(
            collective_id=0, has_side_effects=True, vmem_limit_bytes=60*2**20
        ),
    )(
        mix_input,
        mix_weight,
        expert_input,
        expert_index.T,
        route_share.T,
        norm_gain.reshape(1, width),
        gate_weight,
        up_weight,
        down_weight,
    )


def solution(mesh):
    placed = (
        P("ep", "tp"),
        P(None, "tp"),
        P("ep", "tp"),
        P("ep", None),
        P("ep", None),
        P(),
        P("ep", None, "tp"),
        P("ep", None, "tp"),
        P("ep", None, "tp"),
    )
    return jax.shard_map(
        functools.partial(shards, mesh.shape["ep"], mesh.shape["tp"]),
        mesh=mesh,
        in_specs=placed,
        out_specs=(P("ep", "tp"), P("ep", "tp")),
        check_vma=False,
    )
```
